32 devices in a mesh: fs: 16 (over z, y, x), tp: 2 (over core).
Axes of the slice: x: 2, y: 2, z: 4, core: 2. Of those that a mesh axis runs over, the one named last changes fastest.
Arguments:
- tokens: bfloat16 [6144, 2048], P('fs', 'tp'), may hold values from -24 to 24
- mixer_gain: float32 [2048], replicated, may hold values from 0.1 to 1.9
- pool_input: bfloat16 [2048, 1024], P('fs', 'tp'), may hold values from -0.125 to 0.125
- group_weight: bfloat16 [8, 128, 128], P('tp'), may hold values from -0.5 to 0.5
- channel_scale: float32 [1024], P('tp'), may hold values from 0.5 to 2
- pool_output: bfloat16 [1024, 2048], P('tp', 'fs'), may hold values from -0.1875 to 0.1875
- ffn_gain: float32 [2048], replicated, may hold values from 0.1 to 1.9
- gate_weight: bfloat16 [2048, 5632], P('fs', 'tp'), may hold values from -0.125 to 0.125
- up_weight: bfloat16 [2048, 5632], P('fs', 'tp'), may hold values from -0.125 to 0.125
- down_weight: bfloat16 [5632, 2048], P('tp', 'fs'), may hold values from -0.078125 to 0.078125
- final_gain: float32 [2048], P('tp'), may hold values from 0.1 to 1.9
Outputs:
- normed_out: bfloat16 [6144, 2048], P('fs', 'tp')
The draws below stay inside these ranges and needn't reach their ends.
All inputs are finite; a program needn't handle non-finite values.
Results may differ from the reference program's by a relative error of at most 0.015.
Values may be sent and summed in bfloat16 or wider, within the bound.
A program may use at most 128 MiB of HBM per device.

```python
import math
import jax
import jax.numpy as jnp
from jax import lax

D = 2048
FF = 5632
GROUPS = 8
GROUP_DIM = 128
POOL = 1024
LENGTH = 128
TOKENS = 6144
N_TP = 2


def draw_tokens(key, part):
    base_key, column_key = jax.random.split(jax.random.fold_in(key, 11), 2)
    values = jax.random.normal(base_key, (TOKENS, D), jnp.float32)
    column_scales = jnp.exp(jax.random.uniform(column_key, (8,), jnp.float32, jnp.log(0.3), jnp.log(3.0)))
    values = values * jnp.repeat(column_scales, D // 8)[None, :]
    return jnp.clip(values, -24.0, 24.0).astype(jnp.bfloat16)


def level_of(rng, extent, cuts, least, high):
    level, own = 1.0, jax.random.fold_in(rng, 6)
    for axis_at, parts in cuts:
        heights = jnp.exp(jax.random.uniform(jax.random.fold_in(own, axis_at), (parts,), jnp.float32, least / len(cuts), high / len(cuts)))
        level = level * jnp.repeat(heights, extent[axis_at] // parts).reshape([-1 if axis == axis_at else 1 for axis in range(len(extent))])
    return level


def normal_values(rng, extent, scale, reach, cuts=(), kind=jnp.bfloat16):
    level = level_of(rng, extent, cuts, -0.22, 0.18) if cuts else 1.0
    array = jax.random.normal(rng, extent, jnp.float32) * scale * level
    return jnp.minimum(jnp.maximum(array, -reach), reach).astype(kind)


def setup_inputs(seed: int = 0) -> dict:
    keys = jax.random.split(jax.random.key(seed), 12)
    tokens = draw_tokens(jax.random.fold_in(keys[11], 71), 0)
    mixer_gain = jnp.clip(1.0 + 0.18 * jax.random.normal(keys[1], (D,), jnp.float32), 0.1, 1.9)
    pool_input = normal_values(keys[2], (D, POOL), D ** -0.5, 0.125, ((0, 16), (1, 2)))
    group_weight = normal_values(keys[3], (GROUPS, GROUP_DIM, GROUP_DIM), GROUP_DIM ** -0.5, 0.5, ((0, 2),))
    channel_scale = jnp.clip(jnp.exp(math.log(2.0) - 1.3862944 * jax.random.uniform(keys[4], (POOL,), jnp.float32) ** level_of(keys[4], (POOL,), ((0, 2),), -0.2, 0.2)), 0.5, 2.0)
    pool_output = normal_values(keys[5], (POOL, D), POOL ** -0.5, 0.1875, ((0, 2), (1, 16)))
    ffn_gain = jnp.clip(1.0 + 0.18 * jax.random.normal(keys[6], (D,), jnp.float32), 0.1, 1.9)
    gate_weight = normal_values(keys[7], (D, FF), D ** -0.5, 0.125, ((0, 16), (1, 2)))
    up_weight = normal_values(keys[8], (D, FF), D ** -0.5, 0.125, ((0, 16), (1, 2)))
    down_weight = normal_values(keys[9], (FF, D), FF ** -0.5, 0.078125, ((0, 2), (1, 16)))
    final_gain = jnp.clip(1.0 + 0.18 * jax.random.normal(keys[10], (D,), jnp.float32), 0.1, 1.9)
    return dict(tokens=tokens, mixer_gain=mixer_gain, pool_input=pool_input, group_weight=group_weight, channel_scale=channel_scale, pool_output=pool_output, ffn_gain=ffn_gain, gate_weight=gate_weight, up_weight=up_weight, down_weight=down_weight, final_gain=final_gain)


EPS = 1e-06

def rms(values, gain):
    wide = values.astype(jnp.float32)
    scaled = wide * jax.lax.rsqrt(lax.optimization_barrier(jnp.mean(wide * wide, axis=-1, keepdims=True)) + EPS)
    return scaled * gain.astype(jnp.float32)

def blocked_product(left, right, blocks):
    width = left.shape[1] // blocks
    total = jnp.zeros((left.shape[0], right.shape[1]), jnp.float32)
    for block in range(blocks):
        part = jnp.dot(left[:, block * width:(block + 1) * width], right[block * width:(block + 1) * width], preferred_element_type=jnp.float32)
        total = total + part.astype(jnp.bfloat16).astype(jnp.float32)
    return total

def reference(tokens, mixer_gain, pool_input, group_weight, channel_scale, pool_output, ffn_gain, gate_weight, up_weight, down_weight, final_gain):
    count_rows = tokens.shape[0]
    first_normed = rms(tokens, mixer_gain).astype(jnp.bfloat16)
    pooled_in = jnp.dot(first_normed, pool_input, preferred_element_type=jnp.float32).astype(jnp.bfloat16)
    grid = pooled_in.astype(jnp.float32).reshape(count_rows // LENGTH, LENGTH, GROUPS, GROUP_DIM)
    prefix = jnp.cumsum(grid, axis=1)
    counts = jnp.arange(1, LENGTH + 1, dtype=jnp.float32)[None, :, None]
    pieces = []
    for group in range(GROUPS):
        window = 2 ** (1 + group % 4)
        running = prefix[:, :, group]
        lagged = jnp.pad(running, ((0, 0), (window, 0), (0, 0)))[:, :LENGTH]
        average = (running - lagged) / jnp.minimum(counts, float(window))
        pieces.append(average - grid[:, :, group])
    pooled = jnp.stack(pieces, axis=2).astype(jnp.bfloat16).reshape(count_rows, GROUPS, GROUP_DIM)
    mapped = jnp.einsum('ngc,gcd->ngd', pooled.astype(jnp.float32), group_weight.astype(jnp.float32))
    grouped = (mapped.reshape(count_rows, GROUPS * GROUP_DIM) * channel_scale).astype(jnp.bfloat16)
    mixer_out = blocked_product(grouped, pool_output, N_TP)
    middle = (tokens.astype(jnp.float32) + mixer_out).astype(jnp.bfloat16)
    second_normed = rms(middle, ffn_gain).astype(jnp.bfloat16)
    gate = jnp.dot(second_normed, gate_weight, preferred_element_type=jnp.float32)
    upward = jnp.dot(second_normed, up_weight, preferred_element_type=jnp.float32)
    hidden = (jax.nn.silu(gate) * upward).astype(jnp.bfloat16)
    ffn_out = blocked_product(hidden, down_weight, N_TP)
    closing = middle.astype(jnp.float32) + ffn_out
    return rms(closing, final_gain).astype(jnp.bfloat16)
```

```python
import functools

import jax
import jax.numpy as jnp
from jax import lax
from jax.experimental import pallas as pl
from jax.experimental.pallas import tpu as pltpu
from jax.sharding import Mesh, PartitionSpec as P

GROUP_DIM = 128
LENGTH = 128
EPS = 1e-06
INNER = 4


def partner(at, step, count):
    if count & (count - 1) == 0:
        return at ^ step, at ^ step
    return (at + step) % count, (at - step) % count


def send(value, axis, count, step):
    pairs = [(at, partner(at, step, count)[0]) for at in range(count)]
    return lax.ppermute(value, axis, pairs)


def place(whole, piece, at, dim):
    return lax.dynamic_update_slice_in_dim(whole, piece, at * piece.shape[dim], dim)


def gather(value, axis, dim):
    count = lax.axis_size(axis)
    me = lax.axis_index(axis)
    shape = list(value.shape)
    shape[dim] *= count
    pieces = [(me, value)]
    for step in range(1, count):
        pieces.append((partner(me, step, count)[1], send(value, axis, count, step)))
    whole = jnp.zeros(shape, value.dtype)
    for at, piece in pieces:
        whole = place(whole, piece, at, dim)
    return whole


def exchange(value, axis, cut, dim):
    count = lax.axis_size(axis)
    me = lax.axis_index(axis)
    width = value.shape[cut] // count
    block = lambda at: lax.dynamic_slice_in_dim(value, at * width, width, cut)
    pieces = [(me, block(me))]
    for step in range(1, count):
        there, origin = partner(me, step, count)
        pieces.append((origin, send(block(there), axis, count, step)))
    shape = list(pieces[0][1].shape)
    shape[dim] *= count
    whole = jnp.zeros(shape, value.dtype)
    for at, piece in pieces:
        whole = place(whole, piece, at, dim)
    return whole


def scatter_sum(value, axis, dim):
    count = lax.axis_size(axis)
    me = lax.axis_index(axis)
    width = value.shape[dim] // count
    block = lambda at: lax.dynamic_slice_in_dim(value, at * width, width, dim)
    total = block(me).astype(jnp.float32)
    for step in range(1, count):
        there = partner(me, step, count)[0]
        total = total + send(block(there), axis, count, step).astype(jnp.float32)
    return total


def ring(value, axis, dim, first=None, behind=None):
    count = lax.axis_size(axis)
    me = lax.axis_index(axis)
    shape = list(value.shape)
    shape[dim] *= count
    whole = place(jnp.zeros(shape, value.dtype), value, me, dim)
    ahead = [(at, (at + 1) % count) for at in range(count)]
    back = [(at, (at - 1) % count) for at in range(count)]
    up = down = value
    for step in range(1, count // 2 + 1):
        if step == 1 and first is not None:
            up = first
        else:
            up = lax.ppermute(up, axis, ahead)
        whole = place(whole, up, (me - step) % count, dim)
        if 2 * step < count:
            if step == 1 and behind is not None:
                down = behind
            else:
                down = lax.ppermute(down, axis, back)
            whole = place(whole, down, (me + step) % count, dim)
    return whole


def half_norm(values, gain, width):
    wide = values.astype(jnp.float32)
    squares = lax.psum(jnp.sum(wide * wide, axis=1, keepdims=True), "tp")
    return wide * lax.rsqrt(squares / width + EPS) * gain


def dot(left, right):
    return jnp.dot(left, right, preferred_element_type=jnp.float32)


def local(
    tokens,
    mixer_gain,
    pool_input,
    group_weight,
    channel_scale,
    pool_output,
    ffn_gain,
    gate_weight,
    up_weight,
    down_weight,
    final_gain,
):
    tp = lax.axis_index("tp")
    columns = tokens.shape[1]
    width = columns * lax.axis_size("tp")
    inner = lax.axis_size("inner")

    full_rows = gather(tokens, "tp", 1)
    depth, hidden_all = gate_weight.shape
    hidden_width = hidden_all // inner
    both = jnp.concatenate(
        [
            gate_weight.reshape(depth, inner, hidden_width),
            up_weight.reshape(depth, inner, hidden_width),
        ],
        axis=2,
    ).reshape(depth, inner * 2 * hidden_width)
    pool_in = ring(pool_input[None, None], "outer", 0)
    pool_out = ring(pool_output[None, None], "outer", 0)
    both = exchange(both, "inner", 1, 0)
    pool_in, pool_out, both = lax.optimization_barrier((pool_in, pool_out, both))
    pool_in = gather(pool_in, "inner", 1).reshape(width, pool_input.shape[1])
    down_weight, pool_in = lax.optimization_barrier((down_weight, pool_in))
    pool_out = gather(pool_out, "inner", 1)
    pool_out = jnp.transpose(pool_out, (2, 0, 1, 3)).reshape(pool_output.shape[0], width)
    planes = lax.axis_size("outer")
    first = lax.ppermute(both, "outer", [(at, (at + 1) % planes) for at in range(planes)])
    behind = lax.ppermute(both, "outer", [(at, (at - 1) % planes) for at in range(planes)])
    down = exchange(down_weight, "inner", 0, 1)

    wide = full_rows.astype(jnp.float32)
    first_normed = (
        wide * lax.rsqrt(jnp.mean(wide * wide, axis=-1, keepdims=True) + EPS) * mixer_gain
    ).astype(jnp.bfloat16)
    row_count = first_normed.shape[0]
    pooled_in = dot(first_normed, pool_in).astype(jnp.bfloat16)
    local_groups = group_weight.shape[0]
    group_ids = tp * local_groups + jnp.arange(local_groups, dtype=jnp.int32)
    windows = jnp.left_shift(jnp.int32(2), group_ids % 4)
    later = jnp.arange(LENGTH, dtype=jnp.int32)[None, :, None]
    earlier = jnp.arange(LENGTH, dtype=jnp.int32)[None, None, :]
    reach = windows[:, None, None]
    inside = (earlier <= later) & (earlier > later - reach)
    band = inside.astype(jnp.bfloat16)
    divisor = jnp.minimum(later[:, :, 0] + 1, windows[:, None]).astype(jnp.float32)
    grid_low = pooled_in.reshape(row_count // LENGTH, LENGTH, local_groups, GROUP_DIM)
    window_sums = jnp.einsum("gts,nsgc->ntgc", band, grid_low, preferred_element_type=jnp.float32)
    average = window_sums / jnp.transpose(divisor)[None, :, :, None]
    pooled = (
        (average - grid_low.astype(jnp.float32))
        .astype(jnp.bfloat16)
        .reshape(row_count, local_groups, GROUP_DIM)
    )
    mapped = jnp.einsum("ngc,gcd->ngd", pooled, group_weight, preferred_element_type=jnp.float32)
    grouped = (mapped.reshape(row_count, local_groups * GROUP_DIM) * channel_scale).astype(
        jnp.bfloat16
    )
    mixer_terms = dot(grouped, pool_out).astype(jnp.bfloat16)
    mixer_terms, first, behind, both, down = lax.optimization_barrier(
        (mixer_terms, first, behind, both, down)
    )
    both = ring(both, "outer", 0, first, behind)
    mixer_out = scatter_sum(mixer_terms, "tp", 1)
    middle = (tokens.astype(jnp.float32) + mixer_out).astype(jnp.bfloat16)

    own_gain = lax.dynamic_slice_in_dim(ffn_gain, tp * columns, columns, 0)
    second_half = half_norm(middle, own_gain, width).astype(jnp.bfloat16)
    ahead = lax.ppermute(down, "outer", [(at, (at + 1) % planes) for at in range(planes)])
    after = lax.ppermute(down, "outer", [(at, (at - 1) % planes) for at in range(planes)])
    second_half, both, ahead, after, down = lax.optimization_barrier(
        (gather(second_half, "inner", 0), both, ahead, after, down)
    )
    down = ring(down, "outer", 1, ahead, after)
    second_normed = gather(second_half, "tp", 1)
    gate = dot(second_normed, both[:, :hidden_width])
    upward = dot(second_normed, both[:, hidden_width:])
    hidden = (jax.nn.silu(gate) * upward).astype(jnp.bfloat16)
    ffn_terms = dot(hidden, down).astype(jnp.bfloat16)
    over_cores = scatter_sum(ffn_terms, "tp", 1).astype(jnp.bfloat16)
    ffn_out = scatter_sum(over_cores, "inner", 0)
    closing = middle.astype(jnp.float32) + ffn_out
    return half_norm(closing, final_gain, width).astype(jnp.bfloat16)


def general(mesh):
    fs, tp = mesh.shape["fs"], mesh.shape["tp"]
    inner = INNER if fs % INNER == 0 else 1
    split = Mesh(mesh.devices.reshape(fs // inner, inner, tp), ("outer", "inner", "tp"))
    rows = ("outer", "inner")
    placed = (
        P(rows, "tp"),
        P(),
        P(rows, "tp"),
        P("tp", None, None),
        P("tp"),
        P("tp", rows),
        P(),
        P(rows, "tp"),
        P(rows, "tp"),
        P("tp", rows),
        P("tp"),
    )
    return jax.shard_map(
        local, mesh=split, in_specs=placed, out_specs=P(rows, "tp"), check_vma=False
    )


AXES = ("zh", "zl", "y", "x", "c")
MESH = pl.DeviceIdType.MESH
PIECES = 16


def rel(a=0, b=0, e=0, d=0):
    return 8 * a + 4 * b + 2 * e + d


def kernel(
    tok,
    mixer_gain,
    pin,
    gw,
    cs,
    pout,
    ffn_gain,
    gu,
    dn,
    final_gain,
    out,
    TOKR,
    FN,
    PIN,
    POUT,
    GRP,
    MT,
    MR,
    MID,
    SQS,
    SQR,
    SN,
    GU,
    DN,
    H,
    TS,
    TR,
    OWN,
    S1,
    R1,
    S2,
    R2,
    CL,
    send_sems,
    local_sems,
    r_pin,
    r_pout,
    r_gu,
    r_dn,
    r_misc,
    r_sn,
    r_snc,
    r_tp,
    r_s1,
    r_s2,
):
    at = {name: lax.axis_index(name) for name in AXES}
    zh, zl, y, x, c = (at[name] for name in AXES)
    rows, half = tok.shape
    depth = pin.shape[0]
    hid = dn.shape[1]
    pad = H.shape[2]
    chans = pin.shape[1]
    width = 2 * half
    tile = 256

    def other(*names):
        return tuple(1 - at[n] if n in names else at[n] for n in AXES)

    sent = []

    def push(src, dst, rsem, *names):
        copy = pltpu.make_async_remote_copy(
            src_ref=src,
            dst_ref=dst,
            send_sem=send_sems.at[len(sent)],
            recv_sem=rsem,
            device_id=other(*names),
            device_id_type=MESH,
        )
        copy.start()
        sent.append(copy)

    def got(dst, rsem):
        pltpu.make_async_remote_copy(
            src_ref=dst,
            dst_ref=dst,
            send_sem=send_sems.at[0],
            recv_sem=rsem,
            device_id=other("c"),
            device_id_type=MESH,
        ).wait_recv()

    def bits(a, b, e, d):
        return (
            zh + a * (1 - 2 * zh),
            zl + b * (1 - 2 * zl),
            y + e * (1 - 2 * y),
            x + d * (1 - 2 * x),
        )

    def natural(a, b, e, d):
        h, l, v, u = bits(a, b, e, d)
        return pl.multiple_of((8 * h + 4 * l + 2 * v + u) * depth, depth)

    def grouped_at(a, b, e, d):
        h, l, v, u = bits(a, b, e, d)
        return pl.multiple_of((8 * h + 4 * v + 2 * l + u) * depth, depth)

    def pin_at(*k):
        return PIN.at[pl.ds(natural(*k), depth), :]

    def pout_at(*k):
        return POUT.at[:, pl.ds(natural(*k), depth)]

    def gu_at(*k):
        return GU.at[pl.ds(grouped_at(*k), depth), :]

    def dn_at(*k):
        return DN.at[pl.ds(0, hid), pl.ds(natural(*k), depth)]

    flips = {"zh": (1, 0, 0, 0), "zl": (0, 1, 0, 0), "y": (0, 0, 1, 0), "x": (0, 0, 0, 1)}

    def forward(place, sems, k, names, src=None):
        for name in names:
            there = tuple(p ^ q for p, q in zip(k, flips[name]))
            push(place(*k) if src is None else src, place(*k), sems.at[rel(*there)], name)

    def arrive(place, sems, k):
        got(place(*k), sems.at[rel(*k)])

    DN[pl.ds(hid, pad - hid), :] = jnp.zeros((pad - hid, width), DN.dtype)

    barrier = pltpu.get_barrier_semaphore()
    peers = (("c",), ("x",), ("y",), ("zl",), ("zh",), ("zl", "x"))
    for names in peers:
        pl.semaphore_signal(barrier, inc=1, device_id=other(*names), device_id_type=MESH)
    pl.semaphore_wait(barrier, len(peers))

    mine = (0, 0, 0, 0)
    quarter = 2 * zl + x
    forward(pin_at, r_pin, mine, ("zh", "zl", "x", "y"), pin)
    forward(pout_at, r_pout, mine, ("zh", "zl", "y", "x"), pout)
    push(tok, TOKR, r_misc.at[0], "c")
    forward(gu_at, r_gu, mine, ("zh",), gu.at[quarter])
    locals_ = [
        pltpu.make_async_copy(pin, pin_at(*mine), local_sems.at[0]),
        pltpu.make_async_copy(pout, pout_at(*mine), local_sems.at[1]),
        pltpu.make_async_copy(gu.at[quarter], gu_at(*mine), local_sems.at[2]),
        pltpu.make_async_copy(dn.at[quarter], dn_at(*mine), local_sems.at[3]),
    ]
    for copy in locals_:
        copy.start()

    trades = (((0, 0, 0, 1), ("x",)), ((0, 1, 0, 0), ("zl",)), ((0, 1, 0, 1), ("zl", "x")))

    def trade(place, sems, source, which):
        k, names = which
        _, b, _, d = k
        _, l, _, u = bits(*k)
        push(source.at[2 * l + u], place(*mine), sems.at[rel(*k)], *names)

    trade(gu_at, r_gu, gu, trades[0])
    trade(gu_at, r_gu, gu, trades[1])

    chunk = 16

    got(TOKR, r_misc.at[0])

    @pl.loop(0, rows // chunk)
    def _(i):
        at_rows = pl.ds(pl.multiple_of(i * chunk, chunk), chunk)
        a = tok[at_rows, :].astype(jnp.float32)
        b = TOKR[at_rows, :].astype(jnp.float32)
        mean = (
            jnp.sum(a * a, axis=1, keepdims=True) + jnp.sum(b * b, axis=1, keepdims=True)
        ) / width
        scale = lax.rsqrt(mean + EPS)
        FN[0, at_rows, :] = (a * scale * mixer_gain[c]).astype(FN.dtype)
        FN[1, at_rows, :] = (b * scale * mixer_gain[1 - c]).astype(FN.dtype)

    for k in ((1, 0, 0, 0), (0, 1, 0, 0), (1, 1, 0, 0)):
        down = ("zl",) if k == (1, 0, 0, 0) else ()
        arrive(pin_at, r_pin, k)
        forward(pin_at, r_pin, k, down + ("x", "y"))
        arrive(pout_at, r_pout, k)
        forward(pout_at, r_pout, k, down + ("y", "x"))
    trade(gu_at, r_gu, gu, trades[2])
    for a, b in ((0, 0), (1, 0), (0, 1), (1, 1)):
        arrive(pin_at, r_pin, (a, b, 0, 1))
        forward(pin_at, r_pin, (a, b, 0, 1), ("y",))
        arrive(pout_at, r_pout, (a, b, 1, 0))
        forward(pout_at, r_pout, (a, b, 1, 0), ("x",))
    forward(gu_at, r_gu, mine, ("y",), gu.at[quarter])
    for which in trades[:2]:
        arrive(gu_at, r_gu, which[0])
        forward(gu_at, r_gu, which[0], ("zh", "y"))
    for which in trades:
        trade(dn_at, r_dn, dn, which)
    arrive(gu_at, r_gu, trades[2][0])
    forward(gu_at, r_gu, trades[2][0], ("zh", "y"))
    forward(dn_at, r_dn, mine, ("zh",), dn.at[quarter])
    arrive(gu_at, r_gu, (1, 0, 0, 0))
    forward(gu_at, r_gu, (1, 0, 0, 0), ("y",))

    locals_[0].wait()
    for a, b in ((0, 0), (1, 0), (0, 1), (1, 1)):
        for d in range(2):
            arrive(pin_at, r_pin, (a, b, 1, d))

    groups = gw.shape[0]
    per_tile = tile // GROUP_DIM

    def two_halves(left, weights, columns):
        first = weights[pl.ds(pl.multiple_of(c * half, half), half), columns]
        second = weights[pl.ds(pl.multiple_of((1 - c) * half, half), half), columns]
        return dot(left[0], first) + dot(left[1], second)

    later = lax.broadcasted_iota(jnp.int32, (LENGTH, LENGTH), 0)
    earlier = lax.broadcasted_iota(jnp.int32, (LENGTH, LENGTH), 1)
    place_in = lax.broadcasted_iota(jnp.int32, (LENGTH, GROUP_DIM), 0)
    for n in range(chans // tile):
        pooled_in = two_halves(FN, PIN, slice(n * tile, (n + 1) * tile)).astype(jnp.bfloat16)
        for j in range(per_tile):
            g = n * per_tile + j
            window = 2 << (g % 4)
            band = ((earlier <= later) & (earlier > later - window)).astype(jnp.float32)
            band = band.astype(jnp.bfloat16)
            divisor = jnp.minimum(place_in + 1, window).astype(jnp.float32)
            for s in range(rows // LENGTH):
                grid = pooled_in[s * LENGTH : (s + 1) * LENGTH, j * GROUP_DIM : (j + 1) * GROUP_DIM]
                average = dot(band, grid) / divisor
                pooled = (average - grid.astype(jnp.float32)).astype(jnp.bfloat16)
                mapped = dot(pooled, gw[g])
                GRP[pl.ds(s * LENGTH, LENGTH), pl.ds(g * GROUP_DIM, GROUP_DIM)] = (
                    mapped * cs[:, g * GROUP_DIM : (g + 1) * GROUP_DIM]
                ).astype(GRP.dtype)

    locals_[1].wait()
    for a, b in ((0, 0), (1, 0), (0, 1), (1, 1)):
        for e in range(2):
            arrive(pout_at, r_pout, (a, b, e, 1))

    def cols_of(which, n):
        return pl.ds(pl.multiple_of(which * half + n * tile, tile), tile)

    @pl.loop(0, half // tile)
    def _(n):
        part = dot(GRP[...], POUT[:, cols_of(1 - c, n)])
        MT[:, cols_of(0, n)] = part.astype(MT.dtype)

    push(MT, MR, r_misc.at[1], "c")

    @pl.loop(0, half // tile)
    def _(n):
        part = dot(GRP[...], POUT[:, cols_of(c, n)])
        MID[:, cols_of(0, n)] = part.astype(MID.dtype)

    for which in trades[:1]:
        arrive(dn_at, r_dn, which[0])
        forward(dn_at, r_dn, which[0], ("zh",))
    got(MR, r_misc.at[1])

    @pl.loop(0, rows // chunk)
    def _(i):
        at_rows = pl.ds(pl.multiple_of(i * chunk, chunk), chunk)
        mixed = MID[at_rows, :].astype(jnp.float32) + MR[at_rows, :].astype(jnp.float32)
        middle = (tok[at_rows, :].astype(jnp.float32) + mixed).astype(jnp.bfloat16)
        MID[at_rows, :] = middle
        wide = middle.astype(jnp.float32)
        squares = jnp.sum(wide * wide, axis=1, keepdims=True)
        SQS[0, at_rows, :] = jnp.broadcast_to(squares, (chunk, SQS.shape[2]))

    push(SQS.at[0], SQR.at[0], r_misc.at[2], "c")
    got(SQR.at[0], r_misc.at[2])

    @pl.loop(0, rows // chunk)
    def _(i):
        at_rows = pl.ds(pl.multiple_of(i * chunk, chunk), chunk)
        squares = SQS[0, at_rows, 0:1] + SQR[0, at_rows, 0:1]
        scale = lax.rsqrt(squares / width + EPS)
        wide = MID[at_rows, :].astype(jnp.float32)
        normed = (wide * scale * ffn_gain[c]).astype(SN.dtype)
        for l in range(2):
            for v in range(2):
                source = (4 * l + 2 * v) * depth
                target = (4 * v + 2 * l) * depth
                SN[0, 0, at_rows, pl.ds(target, 2 * depth)] = normed[:, source : source + 2 * depth]

    push(SN.at[0, 0], SN.at[2, 0], r_sn.at[2], "zl")
    push(SN.at[0, 0], SN.at[1, 0], r_sn.at[1], "x")
    push(SN.at[0, 0], SN.at[0, 1], r_snc.at[0], "c")

    arrive(gu_at, r_gu, (1, 0, 0, 1))
    forward(gu_at, r_gu, (1, 0, 0, 1), ("y",))
    for which in trades[1:]:
        arrive(dn_at, r_dn, which[0])
        forward(dn_at, r_dn, which[0], ("zh",))
    got(SN.at[2, 0], r_sn.at[2])
    push(SN.at[2, 0], SN.at[3, 0], r_sn.at[3], "x")
    push(SN.at[2, 0], SN.at[2, 1], r_snc.at[2], "c")
    for k in ((1, 1, 0, 0), (1, 1, 0, 1)):
        arrive(gu_at, r_gu, k)
        forward(gu_at, r_gu, k, ("y",))
    forward(dn_at, r_dn, mine, ("y",), dn.at[quarter])
    for which in trades:
        forward(dn_at, r_dn, which[0], ("y",))
    got(SN.at[1, 0], r_sn.at[1])
    push(SN.at[1, 0], SN.at[1, 1], r_snc.at[1], "c")
    got(SN.at[3, 0], r_sn.at[3])
    push(SN.at[3, 0], SN.at[3, 1], r_snc.at[3], "c")

    locals_[2].wait()
    for a in range(2):
        for b, d in ((0, 0), (0, 1), (1, 0), (1, 1)):
            arrive(gu_at, r_gu, (a, b, 1, d))

    whole_tiles = GU.shape[1] // tile
    lane = lax.broadcasted_iota(jnp.int32, (rows, GROUP_DIM), 1)

    def gated(r):
        @pl.loop(0, whole_tiles)
        def _(j):
            both = two_halves(SN.at[r], GU, pl.ds(pl.multiple_of(j * tile, tile), tile))
            gate, up = both[:, : tile // 2], both[:, tile // 2 :]
            value = gate / (1.0 + jnp.exp(-gate)) * up
            H[r, :, pl.ds(pl.multiple_of(j * (tile // 2), tile // 2), tile // 2)] = value.astype(
                H.dtype
            )

        both = two_halves(SN.at[r], GU, pl.ds(whole_tiles * tile, tile // 2))
        up = pltpu.roll(both, tile // 4, 1)
        value = both / (1.0 + jnp.exp(-both)) * up
        H[r, :, pl.ds(whole_tiles * (tile // 2), tile // 2)] = jnp.where(
            lane < tile // 4, value, 0.0
        ).astype(H.dtype)

    for r, k in ((0, (1, 0, 0, 0)), (2, (1, 0, 0, 1)), (1, (1, 1, 0, 0)), (3, (1, 1, 0, 1))):
        got(SN.at[r, 1], r_snc.at[r])
        gated(r)
        arrive(dn_at, r_dn, k)
        forward(dn_at, r_dn, k, ("y",))

    locals_[3].wait()
    steps = [(l, e) for e in range(2) for l in range(2)]
    firsts = ("x", "zl", "x", "zl")

    def step_cols(s, which):
        l, e = steps[s]
        v = y + e * (1 - 2 * y)
        return pl.ds(pl.multiple_of(which * half + (2 * l + v) * tile, tile), tile)

    def produce(s):
        @pl.loop(0, 4)
        def _(r):
            TS[s, r] = dot(H[r], DN[:, step_cols(s, 1 - c)]).astype(TS.dtype)

        push(TS.at[s], TR.at[s], r_tp.at[s], "c")

        @pl.loop(0, 4)
        def _(r):
            OWN[s % 2, r] = dot(H[r], DN[:, step_cols(s, c)])

    def first_stage(s):
        got(TR.at[s], r_tp.at[s])
        blocks = ((1, 3), (0, 2)) if firsts[s] == "x" else ((2, 3), (0, 1))
        for i, r in enumerate(blocks[0]):
            S1[s, i] = (OWN[s % 2, r] + TR[s, r].astype(jnp.float32)).astype(S1.dtype)
        push(S1.at[s], R1.at[s], r_s1.at[s], firsts[s])
        keep, give = blocks[1]
        CL[0, s] = OWN[s % 2, keep] + TR[s, keep].astype(jnp.float32)
        CL[1, s] = OWN[s % 2, give] + TR[s, give].astype(jnp.float32)

    def second_stage(s):
        got(R1.at[s], r_s1.at[s])
        S2[s] = (CL[1, s] + R1[s, 1].astype(jnp.float32)).astype(S2.dtype)
        push(S2.at[s], R2.at[s], r_s2.at[s], "zl" if firsts[s] == "x" else "x")
        CL[0, s] = CL[0, s] + R1[s, 0].astype(jnp.float32)

    def finish(s, before):
        got(R2.at[s], r_s2.at[s])
        middle = MID[:, step_cols(s, 0)].astype(jnp.float32)
        closing = middle + (CL[0, s] + R2[s].astype(jnp.float32))
        CL[0, s] = closing
        squares = jnp.sum(closing * closing, axis=1, keepdims=True)
        squares = jnp.broadcast_to(squares, SQS.shape[1:])
        SQS[1] = squares if before is None else SQS[1] + squares

    for s in range(4):
        if s % 2 == 0:
            for b in range(2):
                for a in range(2):
                    for d in range(2):
                        if s >= 2:
                            arrive(dn_at, r_dn, (a, b, 1, d))
        produce(s)
        first_stage(s)
        if s >= 1:
            second_stage(s - 1)
        if s >= 2:
            finish(s - 2, None if s == 2 else s)
    second_stage(3)
    finish(2, 2)
    finish(3, 3)
    push(SQS.at[1], SQR.at[1], r_misc.at[3], "c")
    got(SQR.at[1], r_misc.at[3])
    scale = lax.rsqrt((SQS[1, :, 0:1] + SQR[1, :, 0:1]) / width + EPS)
    for s in range(4):
        gain = final_gain[:, step_cols(s, 0)]
        out[:, step_cols(s, 0)] = (CL[0, s] * scale * gain).astype(out.dtype)

    for copy in sent:
        copy.wait_send()


def fused(
    tokens,
    mixer_gain,
    pool_input,
    group_weight,
    channel_scale,
    pool_output,
    ffn_gain,
    gate_weight,
    up_weight,
    down_weight,
    final_gain,
):
    rows, half = tokens.shape
    depth, hidden_all = gate_weight.shape
    hid = hidden_all // 4
    full = hid // GROUP_DIM
    rest = hid - full * GROUP_DIM
    chans = pool_input.shape[1]
    gate4 = jnp.transpose(gate_weight.reshape(depth, 4, hid), (1, 0, 2))
    up4 = jnp.transpose(up_weight.reshape(depth, 4, hid), (1, 0, 2))
    body = full * GROUP_DIM
    pieces = []
    for j in range(full):
        pieces += [gate4[:, :, j * GROUP_DIM : (j + 1) * GROUP_DIM]]
        pieces += [up4[:, :, j * GROUP_DIM : (j + 1) * GROUP_DIM]]
    pieces += [gate4[:, :, body:], up4[:, :, body:]]
    gu = jnp.concatenate(pieces, axis=2)
    dn = down_weight.reshape(4, hid, depth)
    pad = (full + 1) * GROUP_DIM
    bf, f32 = jnp.bfloat16, jnp.float32
    vmem = pl.BlockSpec(memory_space=pltpu.VMEM)
    hbm = pl.BlockSpec(memory_space=pl.ANY)
    dma = pltpu.SemaphoreType.DMA
    tile = 256
    scratch = [
        pltpu.VMEM((rows, half), bf),
        pltpu.VMEM((2, rows, half), bf),
        pltpu.VMEM((2 * half, chans), bf),
        pltpu.VMEM((chans, 2 * half), bf),
        pltpu.VMEM((rows, chans), bf),
        pltpu.VMEM((rows, half), bf),
        pltpu.VMEM((rows, half), bf),
        pltpu.VMEM((rows, half), bf),
        pltpu.VMEM((2, rows, GROUP_DIM), f32),
        pltpu.VMEM((2, rows, GROUP_DIM), f32),
        pltpu.VMEM((4, 2, rows, half), bf),
        pltpu.VMEM((2 * half, 2 * hid), bf),
        pltpu.VMEM((pad, 2 * half), bf),
        pltpu.VMEM((4, rows, pad), bf),
        pltpu.VMEM((4, 4, rows, tile), bf),
        pltpu.VMEM((4, 4, rows, tile), bf),
        pltpu.VMEM((2, 4, rows, tile), f32),
        pltpu.VMEM((4, 2, rows, tile), bf),
        pltpu.VMEM((4, 2, rows, tile), bf),
        pltpu.VMEM((4, rows, tile), bf),
        pltpu.VMEM((4, rows, tile), bf),
        pltpu.VMEM((2, 4, rows, tile), f32),
        dma((96,)),
        dma((4,)),
        dma((PIECES,)),
        dma((PIECES,)),
        dma((PIECES,)),
        dma((PIECES,)),
        dma((4,)),
        dma((4,)),
        dma((4,)),
        dma((4,)),
        dma((4,)),
        dma((4,)),
    ]
    return pl.pallas_call(
        kernel,
        out_shape=jax.ShapeDtypeStruct((rows, half), bf),
        in_specs=[vmem, vmem, hbm, vmem, vmem, hbm, vmem, hbm, hbm, vmem],
        out_specs=vmem,
        scratch_shapes=scratch,
        compiler_params=pltpu.CompilerParams(
            collective_id=0, has_side_effects=True, vmem_limit_bytes=67043328
        ),
    )(
        tokens,
        mixer_gain.reshape(2, 1, half),
        pool_input,
        group_weight,
        channel_scale.reshape(1, chans),
        pool_output,
        ffn_gain.reshape(2, 1, half),
        gu,
        dn,
        final_gain.reshape(1, half),
    )


def solution(mesh):
    fs, tp = mesh.shape["fs"], mesh.shape["tp"]
    if fs != PIECES or tp != 2:
        return general(mesh)
    split = Mesh(mesh.devices.reshape(2, 2, 2, 2, 2), AXES)
    rows = AXES[:4]
    placed = (
        P(rows, "c"),
        P(),
        P(rows, "c"),
        P("c", None, None),
        P("c"),
        P("c", rows),
        P(),
        P(rows, "c"),
        P(rows, "c"),
        P("c", rows),
        P("c"),
    )
    return jax.shard_map(
        fused, mesh=split, in_specs=placed, out_specs=P(rows, "c"), check_vma=False
    )
```

```python
import functools

import jax
import jax.numpy as jnp
from jax import lax
from jax.experimental import pallas as pl
from jax.experimental.pallas import tpu as pltpu
from jax.sharding import Mesh, PartitionSpec as P

GROUP_DIM = 128
LENGTH = 128
EPS = 1e-06
INNER = 4


def partner(at, step, count):
    if count & (count - 1) == 0:
        return at ^ step, at ^ step
    return (at + step) % count, (at - step) % count


def send(value, axis, count, step):
    pairs = [(at, partner(at, step, count)[0]) for at in range(count)]
    return lax.ppermute(value, axis, pairs)


def place(whole, piece, at, dim):
    return lax.dynamic_update_slice_in_dim(whole, piece, at * piece.shape[dim], dim)


def gather(value, axis, dim):
    count = lax.axis_size(axis)
    me = lax.axis_index(axis)
    shape = list(value.shape)
    shape[dim] *= count
    pieces = [(me, value)]
    for step in range(1, count):
        pieces.append((partner(me, step, count)[1], send(value, axis, count, step)))
    whole = jnp.zeros(shape, value.dtype)
    for at, piece in pieces:
        whole = place(whole, piece, at, dim)
    return whole


def exchange(value, axis, cut, dim):
    count = lax.axis_size(axis)
    me = lax.axis_index(axis)
    width = value.shape[cut] // count
    block = lambda at: lax.dynamic_slice_in_dim(value, at * width, width, cut)
    pieces = [(me, block(me))]
    for step in range(1, count):
        there, origin = partner(me, step, count)
        pieces.append((origin, send(block(there), axis, count, step)))
    shape = list(pieces[0][1].shape)
    shape[dim] *= count
    whole = jnp.zeros(shape, value.dtype)
    for at, piece in pieces:
        whole = place(whole, piece, at, dim)
    return whole


def scatter_sum(value, axis, dim):
    count = lax.axis_size(axis)
    me = lax.axis_index(axis)
    width = value.shape[dim] // count
    block = lambda at: lax.dynamic_slice_in_dim(value, at * width, width, dim)
    total = block(me).astype(jnp.float32)
    for step in range(1, count):
        there = partner(me, step, count)[0]
        total = total + send(block(there), axis, count, step).astype(jnp.float32)
    return total


def ring(value, axis, dim, first=None, behind=None):
    count = lax.axis_size(axis)
    me = lax.axis_index(axis)
    shape = list(value.shape)
    shape[dim] *= count
    whole = place(jnp.zeros(shape, value.dtype), value, me, dim)
    ahead = [(at, (at + 1) % count) for at in range(count)]
    back = [(at, (at - 1) % count) for at in range(count)]
    up = down = value
    for step in range(1, count // 2 + 1):
        if step == 1 and first is not None:
            up = first
        else:
            up = lax.ppermute(up, axis, ahead)
        whole = place(whole, up, (me - step) % count, dim)
        if 2 * step < count:
            if step == 1 and behind is not None:
                down = behind
            else:
                down = lax.ppermute(down, axis, back)
            whole = place(whole, down, (me + step) % count, dim)
    return whole


def half_norm(values, gain, width):
    wide = values.astype(jnp.float32)
    squares = lax.psum(jnp.sum(wide * wide, axis=1, keepdims=True), "tp")
    return wide * lax.rsqrt(squares / width + EPS) * gain


def dot(left, right):
    return jnp.dot(left, right, preferred_element_type=jnp.float32)


def local(
    tokens,
    mixer_gain,
    pool_input,
    group_weight,
    channel_scale,
    pool_output,
    ffn_gain,
    gate_weight,
    up_weight,
    down_weight,
    final_gain,
):
    tp = lax.axis_index("tp")
    columns = tokens.shape[1]
    width = columns * lax.axis_size("tp")
    inner = lax.axis_size("inner")

    full_rows = gather(tokens, "tp", 1)
    depth, hidden_all = gate_weight.shape
    hidden_width = hidden_all // inner
    both = jnp.concatenate(
        [
            gate_weight.reshape(depth, inner, hidden_width),
            up_weight.reshape(depth, inner, hidden_width),
        ],
        axis=2,
    ).reshape(depth, inner * 2 * hidden_width)
    pool_in = ring(pool_input[None, None], "outer", 0)
    pool_out = ring(pool_output[None, None], "outer", 0)
    both = exchange(both, "inner", 1, 0)
    pool_in, pool_out, both = lax.optimization_barrier((pool_in, pool_out, both))
    pool_in = gather(pool_in, "inner", 1).reshape(width, pool_input.shape[1])
    down_weight, pool_in = lax.optimization_barrier((down_weight, pool_in))
    pool_out = gather(pool_out, "inner", 1)
    pool_out = jnp.transpose(pool_out, (2, 0, 1, 3)).reshape(pool_output.shape[0], width)
    planes = lax.axis_size("outer")
    first = lax.ppermute(both, "outer", [(at, (at + 1) % planes) for at in range(planes)])
    behind = lax.ppermute(both, "outer", [(at, (at - 1) % planes) for at in range(planes)])
    down = exchange(down_weight, "inner", 0, 1)

    wide = full_rows.astype(jnp.float32)
    first_normed = (
        wide * lax.rsqrt(jnp.mean(wide * wide, axis=-1, keepdims=True) + EPS) * mixer_gain
    ).astype(jnp.bfloat16)
    row_count = first_normed.shape[0]
    pooled_in = dot(first_normed, pool_in).astype(jnp.bfloat16)
    local_groups = group_weight.shape[0]
    group_ids = tp * local_groups + jnp.arange(local_groups, dtype=jnp.int32)
    windows = jnp.left_shift(jnp.int32(2), group_ids % 4)
    later = jnp.arange(LENGTH, dtype=jnp.int32)[None, :, None]
    earlier = jnp.arange(LENGTH, dtype=jnp.int32)[None, None, :]
    reach = windows[:, None, None]
    inside = (earlier <= later) & (earlier > later - reach)
    band = inside.astype(jnp.bfloat16)
    divisor = jnp.minimum(later[:, :, 0] + 1, windows[:, None]).astype(jnp.float32)
    grid_low = pooled_in.reshape(row_count // LENGTH, LENGTH, local_groups, GROUP_DIM)
    window_sums = jnp.einsum("gts,nsgc->ntgc", band, grid_low, preferred_element_type=jnp.float32)
    average = window_sums / jnp.transpose(divisor)[None, :, :, None]
    pooled = (
        (average - grid_low.astype(jnp.float32))
        .astype(jnp.bfloat16)
        .reshape(row_count, local_groups, GROUP_DIM)
    )
    mapped = jnp.einsum("ngc,gcd->ngd", pooled, group_weight, preferred_element_type=jnp.float32)
    grouped = (mapped.reshape(row_count, local_groups * GROUP_DIM) * channel_scale).astype(
        jnp.bfloat16
    )
    mixer_terms = dot(grouped, pool_out).astype(jnp.bfloat16)
    mixer_terms, first, behind, both, down = lax.optimization_barrier(
        (mixer_terms, first, behind, both, down)
    )
    both = ring(both, "outer", 0, first, behind)
    mixer_out = scatter_sum(mixer_terms, "tp", 1)
    middle = (tokens.astype(jnp.float32) + mixer_out).astype(jnp.bfloat16)

    own_gain = lax.dynamic_slice_in_dim(ffn_gain, tp * columns, columns, 0)
    second_half = half_norm(middle, own_gain, width).astype(jnp.bfloat16)
    ahead = lax.ppermute(down, "outer", [(at, (at + 1) % planes) for at in range(planes)])
    after = lax.ppermute(down, "outer", [(at, (at - 1) % planes) for at in range(planes)])
    second_half, both, ahead, after, down = lax.optimization_barrier(
        (gather(second_half, "inner", 0), both, ahead, after, down)
    )
    down = ring(down, "outer", 1, ahead, after)
    second_normed = gather(second_half, "tp", 1)
    gate = dot(second_normed, both[:, :hidden_width])
    upward = dot(second_normed, both[:, hidden_width:])
    hidden = (jax.nn.silu(gate) * upward).astype(jnp.bfloat16)
    ffn_terms = dot(hidden, down).astype(jnp.bfloat16)
    over_cores = scatter_sum(ffn_terms, "tp", 1).astype(jnp.bfloat16)
    ffn_out = scatter_sum(over_cores, "inner", 0)
    closing = middle.astype(jnp.float32) + ffn_out
    return half_norm(closing, final_gain, width).astype(jnp.bfloat16)


def general(mesh):
    fs, tp = mesh.shape["fs"], mesh.shape["tp"]
    inner = INNER if fs % INNER == 0 else 1
    split = Mesh(mesh.devices.reshape(fs // inner, inner, tp), ("outer", "inner", "tp"))
    rows = ("outer", "inner")
    placed = (
        P(rows, "tp"),
        P(),
        P(rows, "tp"),
        P("tp", None, None),
        P("tp"),
        P("tp", rows),
        P(),
        P(rows, "tp"),
        P(rows, "tp"),
        P("tp", rows),
        P("tp"),
    )
    return jax.shard_map(
        local, mesh=split, in_specs=placed, out_specs=P(rows, "tp"), check_vma=False
    )


AXES = ("zh", "zl", "y", "x", "c")
MESH = pl.DeviceIdType.MESH
PIECES = 16


def rel(a=0, b=0, e=0, d=0):
    return 8 * a + 4 * b + 2 * e + d


def kernel(
    tok,
    mixer_gain,
    pin,
    gw,
    cs,
    pout,
    ffn_gain,
    gu,
    dn,
    final_gain,
    out,
    TOKR,
    FN,
    PIN,
    POUT,
    GRP,
    MT,
    MR,
    MID,
    SQS,
    SQR,
    SN,
    GU,
    DN,
    ACC,
    H,
    TS,
    TR,
    OWN,
    S1,
    R1,
    S2,
    R2,
    CL,
    send_sems,
    local_sems,
    r_pin,
    r_pout,
    r_gu,
    r_dn,
    r_misc,
    r_sn,
    r_snc,
    r_tp,
    r_s1,
    r_s2,
):
    at = {name: lax.axis_index(name) for name in AXES}
    zh, zl, y, x, c = (at[name] for name in AXES)
    rows, half = tok.shape
    depth = pin.shape[0]
    hid = dn.shape[1]
    pad = H.shape[2]
    chans = pin.shape[1]
    width = 2 * half
    tile = 256

    fold = zl + zh - 2 * zl * zh

    def other(*names):
        flip = {n: n in names for n in AXES}
        flip["zl"] = flip["zl"] != flip["zh"]
        return tuple(1 - at[n] if flip[n] else at[n] for n in AXES)

    sent = []
    count = [0]

    def prepare(src, dst, rsem, *names):
        copy = pltpu.make_async_remote_copy(
            src_ref=src,
            dst_ref=dst,
            send_sem=send_sems.at[count[0]],
            recv_sem=rsem,
            device_id=other(*names),
            device_id_type=MESH,
        )
        count[0] += 1
        sent.append(copy)
        return copy

    def push(src, dst, rsem, *names):
        prepare(src, dst, rsem, *names).start()

    def got(dst, rsem, name):
        with jax.named_scope("wait_" + name):
            pltpu.make_async_remote_copy(
                src_ref=dst,
                dst_ref=dst,
                send_sem=send_sems.at[0],
                recv_sem=rsem,
                device_id=other("c"),
                device_id_type=MESH,
            ).wait_recv()

    def bits(a, b, e, d):
        m = b if a == 0 else 1 - b
        return (
            zh + a * (1 - 2 * zh),
            zl + m * (1 - 2 * zl),
            y + e * (1 - 2 * y),
            x + d * (1 - 2 * x),
        )

    def natural(a, b, e, d):
        h, l, v, u = bits(a, b, e, d)
        return pl.multiple_of((8 * h + 4 * l + 2 * v + u) * depth, depth)

    def grouped_at(a, b, e, d):
        h, l, v, u = bits(a, b, e, d)
        return pl.multiple_of((8 * h + 4 * v + 2 * l + u) * depth, depth)

    def pin_at(*k):
        return PIN.at[pl.ds(natural(*k), depth), :]

    def pout_at(*k):
        return POUT.at[:, pl.ds(natural(*k), depth)]

    def gu_at(*k):
        return GU.at[pl.ds(grouped_at(*k), depth), :]

    def dn_at(*k):
        return DN.at[pl.ds(0, hid), pl.ds(natural(*k), depth)]

    flips = {"zh": (1, 0, 0, 0), "zl": (0, 1, 0, 0), "y": (0, 0, 1, 0), "x": (0, 0, 0, 1)}

    def forward(place, sems, k, names, src=None):
        for name in names:
            there = tuple(1 - p if q else p for p, q in zip(k, flips[name]))
            push(place(*k) if src is None else src, place(*k), sems.at[rel(*there)], name)

    def start_if(condition, copy):
        @pl.when(condition)
        def _():
            copy.start()

    def arrive(place, sems, k):
        name = place.__name__ + "".join(str(bit) if isinstance(bit, int) else "v" for bit in k)
        got(place(*k), sems.at[rel(*k)], name)

    DN[pl.ds(hid, pad - hid), :] = jnp.zeros((pad - hid, width), DN.dtype)

    barrier = pltpu.get_barrier_semaphore()
    peers = (("c",), ("x",), ("y",), ("zl",), ("zh",), ("zl", "x"))
    for names in peers:
        pl.semaphore_signal(barrier, inc=1, device_id=other(*names), device_id_type=MESH)
    with jax.named_scope("barrier"):
        pl.semaphore_wait(barrier, len(peers))

    mine = (0, 0, 0, 0)
    quarter = 2 * fold + x
    push(tok, TOKR, r_misc.at[0], "c")
    forward(pin_at, r_pin, mine, ("zh", "zl", "x", "y"), pin)
    forward(pout_at, r_pout, mine, ("zh", "zl", "y", "x"), pout)
    own_over = prepare(gu.at[quarter], gu_at(*mine), r_gu.at[rel(a=1)], "zh")
    start_if(fold == 1, own_over)
    locals_ = [
        pltpu.make_async_copy(pin, pin_at(*mine), local_sems.at[0]),
        pltpu.make_async_copy(pout, pout_at(*mine), local_sems.at[1]),
        pltpu.make_async_copy(gu.at[quarter], gu_at(*mine), local_sems.at[2]),
        pltpu.make_async_copy(dn.at[quarter], dn_at(*mine), local_sems.at[3]),
    ]
    for copy in locals_:
        copy.start()

    trades = (((0, 0, 0, 1), ("x",)), ((0, 1, 0, 0), ("zl",)), ((0, 1, 0, 1), ("zl", "x")))

    def trade(place, sems, source, which):
        k, names = which
        _, b, _, d = k
        there = 2 * (1 - fold if b else fold) + (1 - x if d else x)
        push(source.at[there], place(*mine), sems.at[rel(*k)], *names)

    def low(l, a=0):
        return zl if l == a else 1 - zl

    chunk = 16

    def normalize():
        got(TOKR, r_misc.at[0], "tok")

        @pl.loop(0, rows // chunk)
        def _(i):
            at_rows = pl.ds(pl.multiple_of(i * chunk, chunk), chunk)
            a = tok[at_rows, :].astype(jnp.float32)
            b = TOKR[at_rows, :].astype(jnp.float32)
            mean = (
                jnp.sum(a * a, axis=1, keepdims=True) + jnp.sum(b * b, axis=1, keepdims=True)
            ) / width
            scale = lax.rsqrt(mean + EPS)
            FN[0, at_rows, :] = (a * scale * mixer_gain[c]).astype(FN.dtype)
            FN[1, at_rows, :] = (b * scale * mixer_gain[1 - c]).astype(FN.dtype)

    def across(a, b):
        arrive(pin_at, r_pin, (a, b, 0, 1))
        forward(pin_at, r_pin, (a, b, 0, 1), ("y",))
        arrive(pout_at, r_pout, (a, b, 1, 0))
        forward(pout_at, r_pout, (a, b, 1, 0), ("x",))

    across(0, 0)
    arrive(pin_at, r_pin, (1, 0, 0, 0))
    forward(pin_at, r_pin, (1, 0, 0, 0), ("zl", "x", "y"))
    arrive(pout_at, r_pout, (1, 0, 0, 0))
    forward(pout_at, r_pout, (1, 0, 0, 0), ("zl", "y", "x"))
    for k in ((0, 1, 0, 0), (1, 1, 0, 0)):
        arrive(pin_at, r_pin, k)
        forward(pin_at, r_pin, k, ("x", "y"))
        arrive(pout_at, r_pout, k)
        forward(pout_at, r_pout, k, ("y", "x"))
    trade(gu_at, r_gu, gu, trades[1])
    start_if(fold == 0, own_over)
    normalize()
    for a, b in ((1, 0), (0, 1), (1, 1)):
        across(a, b)
    forward(gu_at, r_gu, mine, ("y",), gu.at[quarter])
    arrive(gu_at, r_gu, trades[1][0])
    forward(gu_at, r_gu, trades[1][0], ("zh", "y"))

    locals_[0].wait()
    for a, b in ((0, 0), (1, 0), (0, 1), (1, 1)):
        for d in range(2):
            arrive(pin_at, r_pin, (a, b, 1, d))
    trade(gu_at, r_gu, gu, trades[0])
    trade(gu_at, r_gu, gu, trades[2])
    trade(dn_at, r_dn, dn, trades[1])

    groups = gw.shape[0]
    per_tile = tile // GROUP_DIM

    def two_halves(left, weights, columns):
        first = weights[pl.ds(pl.multiple_of(c * half, half), half), columns]
        second = weights[pl.ds(pl.multiple_of((1 - c) * half, half), half), columns]
        return dot(left[0], first) + dot(left[1], second)

    later = lax.broadcasted_iota(jnp.int32, (LENGTH, LENGTH), 0)
    earlier = lax.broadcasted_iota(jnp.int32, (LENGTH, LENGTH), 1)
    place_in = lax.broadcasted_iota(jnp.int32, (LENGTH, GROUP_DIM), 0)
    for n in range(chans // tile):
        pooled_in = two_halves(FN, PIN, slice(n * tile, (n + 1) * tile)).astype(jnp.bfloat16)
        for j in range(per_tile):
            g = n * per_tile + j
            window = 2 << (g % 4)
            band = ((earlier <= later) & (earlier > later - window)).astype(jnp.float32)
            band = band.astype(jnp.bfloat16)
            divisor = jnp.minimum(place_in + 1, window).astype(jnp.float32)
            for s in range(rows // LENGTH):
                grid = pooled_in[s * LENGTH : (s + 1) * LENGTH, j * GROUP_DIM : (j + 1) * GROUP_DIM]
                average = dot(band, grid) / divisor
                pooled = (average - grid.astype(jnp.float32)).astype(jnp.bfloat16)
                mapped = dot(pooled, gw[g])
                GRP[pl.ds(s * LENGTH, LENGTH), pl.ds(g * GROUP_DIM, GROUP_DIM)] = (
                    mapped * cs[:, g * GROUP_DIM : (g + 1) * GROUP_DIM]
                ).astype(GRP.dtype)

    locals_[1].wait()
    for a, b in ((0, 0), (1, 0), (0, 1), (1, 1)):
        for e in range(2):
            arrive(pout_at, r_pout, (a, b, e, 1))

    def cols_of(which, n):
        return pl.ds(pl.multiple_of(which * half + n * tile, tile), tile)

    @pl.loop(0, half // tile)
    def _(n):
        part = dot(GRP[...], POUT[:, cols_of(1 - c, n)])
        MT[:, cols_of(0, n)] = part.astype(MT.dtype)

    push(MT, MR, r_misc.at[1], "c")

    @pl.loop(0, half // tile)
    def _(n):
        part = dot(GRP[...], POUT[:, cols_of(c, n)])
        MID[:, cols_of(0, n)] = part.astype(MID.dtype)

    arrive(gu_at, r_gu, (1, 0, 0, 0))
    forward(gu_at, r_gu, (1, 0, 0, 0), ("y",))
    got(MR, r_misc.at[1], "mix")

    @pl.loop(0, rows // chunk)
    def _(i):
        at_rows = pl.ds(pl.multiple_of(i * chunk, chunk), chunk)
        mixed = MID[at_rows, :].astype(jnp.float32) + MR[at_rows, :].astype(jnp.float32)
        middle = (tok[at_rows, :].astype(jnp.float32) + mixed).astype(jnp.bfloat16)
        MID[at_rows, :] = middle
        wide = middle.astype(jnp.float32)
        squares = jnp.sum(wide * wide, axis=1, keepdims=True)
        SQS[0, at_rows, :] = jnp.broadcast_to(squares, (chunk, SQS.shape[2]))

    push(SQS.at[0], SQR.at[0], r_misc.at[2], "c")
    got(SQR.at[0], r_misc.at[2], "sq0")

    @pl.loop(0, rows // chunk)
    def _(i):
        at_rows = pl.ds(pl.multiple_of(i * chunk, chunk), chunk)
        squares = SQS[0, at_rows, 0:1] + SQR[0, at_rows, 0:1]
        scale = lax.rsqrt(squares / width + EPS)
        wide = MID[at_rows, :].astype(jnp.float32)
        normed = (wide * scale * ffn_gain[c]).astype(SN.dtype)
        for l in range(2):
            for v in range(2):
                source = (4 * l + 2 * v) * depth
                target = (4 * v + 2 * l) * depth
                SN[0, 0, at_rows, pl.ds(target, 2 * depth)] = normed[:, source : source + 2 * depth]

    push(SN.at[0, 0], SN.at[2, 0], r_sn.at[2], "zl")
    push(SN.at[0, 0], SN.at[1, 0], r_sn.at[1], "x")
    push(SN.at[0, 0], SN.at[0, 1], r_snc.at[0], "c")

    trade(dn_at, r_dn, dn, trades[0])
    trade(dn_at, r_dn, dn, trades[2])
    for i in (0, 2):
        arrive(gu_at, r_gu, trades[i][0])
        forward(gu_at, r_gu, trades[i][0], ("zh", "y"))
    arrive(gu_at, r_gu, (1, 1, 0, 0))
    forward(gu_at, r_gu, (1, 1, 0, 0), ("y",))
    got(SN.at[1, 0], r_sn.at[1], "sn1")
    push(SN.at[1, 0], SN.at[1, 1], r_snc.at[1], "c")
    got(SN.at[2, 0], r_sn.at[2], "sn2")
    push(SN.at[2, 0], SN.at[3, 0], r_sn.at[3], "x")
    push(SN.at[2, 0], SN.at[2, 1], r_snc.at[2], "c")
    locals_[3].wait()
    for which in trades:
        arrive(dn_at, r_dn, which[0])
    for l in range(2):
        for d in range(2):
            forward(dn_at, r_dn, (0, low(l), 0, d), ("zh",))

    whole_tiles = GU.shape[1] // tile
    half_tile = tile // 2
    lane = lax.broadcasted_iota(jnp.int32, (rows, half_tile), 1)
    near = jnp.where(zh == c, 0, 1)
    near_rows = pl.ds(pl.multiple_of(zh * half, half), half)
    far_rows = pl.ds(pl.multiple_of((1 - zh) * half, half), half)
    last = pl.ds(whole_tiles * tile, half_tile)

    def tile_at(j, size):
        return pl.ds(pl.multiple_of(j * size, size), size)

    def begin(r):
        got(SN.at[r, 1], r_snc.at[r], f"snc{r}")
        with jax.named_scope(f"begin{r}"):

            @pl.loop(0, whole_tiles)
            def _(j):
                ACC[r, :, tile_at(j, tile)] = dot(SN[r, near], GU[near_rows, tile_at(j, tile)])

            ACC[r, :, last] = dot(SN[r, near], GU[near_rows, last])

    def gated(r):
        with jax.named_scope(f"gated{r}"):

            @pl.loop(0, whole_tiles)
            def _(j):
                both = dot(SN[r, 1 - near], GU[far_rows, tile_at(j, tile)])
                both = both + ACC[r, :, tile_at(j, tile)]
                gate, up = both[:, :half_tile], both[:, half_tile:]
                value = gate / (1.0 + jnp.exp(-gate)) * up
                H[r, :, tile_at(j, half_tile)] = value.astype(H.dtype)

            both = dot(SN[r, 1 - near], GU[far_rows, last]) + ACC[r, :, last]
            up = pltpu.roll(both, half_tile // 2, 1)
            value = both / (1.0 + jnp.exp(-both)) * up
            H[r, :, pl.ds(whole_tiles * half_tile, half_tile)] = jnp.where(
                lane < half_tile // 2, value, 0.0
            ).astype(H.dtype)

    locals_[2].wait()
    for b, d in ((0, 0), (0, 1), (1, 0), (1, 1)):
        arrive(gu_at, r_gu, (0, b, 1, d))
    begin(0)
    arrive(gu_at, r_gu, (1, 0, 0, 1))
    forward(gu_at, r_gu, (1, 0, 0, 1), ("y",))
    begin(1)
    begin(2)
    arrive(gu_at, r_gu, (1, 1, 0, 1))
    forward(gu_at, r_gu, (1, 1, 0, 1), ("y",))
    for l in range(2):
        for d in range(2):
            forward(dn_at, r_dn, (0, low(l), 0, d), ("y",))
    got(SN.at[3, 0], r_sn.at[3], "sn3")
    push(SN.at[3, 0], SN.at[3, 1], r_snc.at[3], "c")
    begin(3)
    for b, d in ((0, 0), (0, 1), (1, 0), (1, 1)):
        arrive(gu_at, r_gu, (1, b, 1, d))
    for r in range(4):
        gated(r)

    steps = [(a, e, l) for a in range(2) for e in range(2) for l in range(2)]
    firsts = ("x", "zl")
    owners = (zh == c, zh != c)
    role_sent = ([], [])

    def role_copy(which, *args):
        copy = prepare(*args)
        sent.pop()
        role_sent[which].append(copy)
        return copy

    def step_cols(s, which=0):
        _, e, l = steps[s]
        v = y + e * (1 - 2 * y)
        return pl.ds(pl.multiple_of(which * half + (2 * l + v) * tile, tile), tile)

    def produce(s):
        a, t = steps[s][0], s % 4
        columns = step_cols(s, zh + a * (1 - 2 * zh))
        over = role_copy(1 - a, TS.at[t], TR.at[t], r_tp.at[t], "c")

        @pl.when(owners[1 - a])
        def _():
            @pl.loop(0, 4)
            def _(r):
                TS[t, r] = dot(H[r], DN[:, columns]).astype(TS.dtype)

            over.start()

        @pl.when(owners[a])
        def _():
            @pl.loop(0, 4)
            def _(r):
                OWN[s % 2, r] = dot(H[r], DN[:, columns])

    def first_stage(s):
        a, t = steps[s][0], s % 4
        axis = firsts[s % 2]
        over = role_copy(a, S1.at[t], R1.at[t], r_s1.at[t], axis)

        @pl.when(owners[a])
        def _():
            got(TR.at[t], r_tp.at[t], f"tp{s}")
            blocks = ((1, 3), (0, 2)) if axis == "x" else ((2, 3), (0, 1))
            for i, r in enumerate(blocks[0]):
                S1[t, i] = (OWN[s % 2, r] + TR[t, r].astype(jnp.float32)).astype(S1.dtype)
            over.start()
            keep, give = blocks[1]
            CL[0, t] = OWN[s % 2, keep] + TR[t, keep].astype(jnp.float32)
            CL[1, t] = OWN[s % 2, give] + TR[t, give].astype(jnp.float32)

    def second_stage(s):
        a, t = steps[s][0], s % 4
        axis = firsts[1 - s % 2]
        over = role_copy(a, S2.at[t], R2.at[t], r_s2.at[t], axis)

        @pl.when(owners[a])
        def _():
            got(R1.at[t], r_s1.at[t], f"first{s}")
            S2[t] = (CL[1, t] + R1[t, 1].astype(jnp.float32)).astype(S2.dtype)
            over.start()
            CL[0, t] = CL[0, t] + R1[t, 0].astype(jnp.float32)

    def finish(s):
        a, t = steps[s][0], s % 4
        columns = step_cols(s)

        @pl.when(owners[a])
        def _():
            got(R2.at[t], r_s2.at[t], f"second{s}")
            middle = MID[:, columns].astype(jnp.float32)
            closing = middle + (CL[0, t] + R2[t].astype(jnp.float32))
            CL[0, t] = closing
            squares = jnp.sum(closing * closing, axis=1, keepdims=True)
            squares = jnp.broadcast_to(squares, SQS.shape[1:])
            SQS[1] = squares if t == 0 else SQS[1] + squares

    def relay(l):
        for d in range(2):
            k = (1, low(l, 1), 0, d)
            arrive(dn_at, r_dn, k)
            forward(dn_at, r_dn, k, ("y",))

    def landed(a, l):
        for d in range(2):
            arrive(dn_at, r_dn, (a, low(l, a), 1, d))

    produce(0)
    produce(1)
    first_stage(0)
    first_stage(1)
    relay(0)
    landed(0, 0)
    produce(2)
    landed(0, 1)
    produce(3)
    second_stage(0)
    second_stage(1)
    first_stage(2)
    first_stage(3)
    produce(4)
    relay(1)
    produce(5)
    first_stage(4)
    first_stage(5)
    finish(0)
    finish(1)
    second_stage(2)
    second_stage(3)
    landed(1, 0)
    produce(6)
    landed(1, 1)
    produce(7)
    second_stage(4)
    second_stage(5)
    first_stage(6)
    first_stage(7)
    finish(2)
    finish(3)
    finish(4)
    finish(5)
    for s in (6, 7):
        second_stage(s)
    for s in (6, 7):
        finish(s)
    push(SQS.at[1], SQR.at[1], r_misc.at[3], "c")
    got(SQR.at[1], r_misc.at[3], "sq1")
    scale = lax.rsqrt((SQS[1, :, 0:1] + SQR[1, :, 0:1]) / width + EPS)
    for s in range(4):
        gain = final_gain[:, step_cols(s)]
        out[:, step_cols(s)] = (CL[0, s] * scale * gain).astype(out.dtype)

    with jax.named_scope("drain"):
        for copy in sent:
            copy.wait_send()
        for which in range(2):

            @pl.when(owners[which])
            def _():
                for copy in role_sent[which]:
                    copy.wait_send()


def fused(
    tokens,
    mixer_gain,
    pool_input,
    group_weight,
    channel_scale,
    pool_output,
    ffn_gain,
    gate_weight,
    up_weight,
    down_weight,
    final_gain,
):
    rows, half = tokens.shape
    depth, hidden_all = gate_weight.shape
    hid = hidden_all // 4
    full = hid // GROUP_DIM
    rest = hid - full * GROUP_DIM
    chans = pool_input.shape[1]
    gate4 = jnp.transpose(gate_weight.reshape(depth, 4, hid), (1, 0, 2))
    up4 = jnp.transpose(up_weight.reshape(depth, 4, hid), (1, 0, 2))
    body = full * GROUP_DIM
    pieces = []
    for j in range(full):
        pieces += [gate4[:, :, j * GROUP_DIM : (j + 1) * GROUP_DIM]]
        pieces += [up4[:, :, j * GROUP_DIM : (j + 1) * GROUP_DIM]]
    pieces += [gate4[:, :, body:], up4[:, :, body:]]
    gu = jnp.concatenate(pieces, axis=2)
    dn = down_weight.reshape(4, hid, depth)
    pad = (full + 1) * GROUP_DIM
    bf, f32 = jnp.bfloat16, jnp.float32
    vmem = pl.BlockSpec(memory_space=pltpu.VMEM)
    hbm = pl.BlockSpec(memory_space=pl.ANY)
    dma = pltpu.SemaphoreType.DMA
    tile = 256
    scratch = [
        pltpu.VMEM((rows, half), bf),
        pltpu.VMEM((2, rows, half), bf),
        pltpu.VMEM((2 * half, chans), bf),
        pltpu.VMEM((chans, 2 * half), bf),
        pltpu.VMEM((rows, chans), bf),
        pltpu.VMEM((rows, half), bf),
        pltpu.VMEM((rows, half), bf),
        pltpu.VMEM((rows, half), bf),
        pltpu.VMEM((2, rows, GROUP_DIM), f32),
        pltpu.VMEM((2, rows, GROUP_DIM), f32),
        pltpu.VMEM((4, 2, rows, half), bf),
        pltpu.VMEM((2 * half, 2 * hid), bf),
        pltpu.VMEM((pad, 2 * half), bf),
        pltpu.VMEM((4, rows, 2 * hid), f32),
        pltpu.VMEM((4, rows, pad), bf),
        pltpu.VMEM((4, 4, rows, tile), bf),
        pltpu.VMEM((4, 4, rows, tile), bf),
        pltpu.VMEM((2, 4, rows, tile), f32),
        pltpu.VMEM((4, 2, rows, tile), bf),
        pltpu.VMEM((4, 2, rows, tile), bf),
        pltpu.VMEM((4, rows, tile), bf),
        pltpu.VMEM((4, rows, tile), bf),
        pltpu.VMEM((2, 4, rows, tile), f32),
        dma((128,)),
        dma((4,)),
        dma((PIECES,)),
        dma((PIECES,)),
        dma((PIECES,)),
        dma((PIECES,)),
        dma((4,)),
        dma((4,)),
        dma((4,)),
        dma((4,)),
        dma((4,)),
        dma((4,)),
    ]
    return pl.pallas_call(
        kernel,
        out_shape=jax.ShapeDtypeStruct((rows, half), bf),
        in_specs=[vmem, vmem, hbm, vmem, vmem, hbm, vmem, hbm, hbm, vmem],
        out_specs=vmem,
        scratch_shapes=scratch,
        compiler_params=pltpu.CompilerParams(
            collective_id=0, has_side_effects=True, vmem_limit_bytes=67043328
        ),
    )(
        tokens,
        mixer_gain.reshape(2, 1, half),
        pool_input,
        group_weight,
        channel_scale.reshape(1, chans),
        pool_output,
        ffn_gain.reshape(2, 1, half),
        gu,
        dn,
        final_gain.reshape(1, half),
    )


def solution(mesh):
    fs, tp = mesh.shape["fs"], mesh.shape["tp"]
    if fs != PIECES or tp != 2:
        return general(mesh)
    split = Mesh(mesh.devices.reshape(2, 2, 2, 2, 2), AXES)
    rows = AXES[:4]
    placed = (
        P(rows, "c"),
        P(),
        P(rows, "c"),
        P("c", None, None),
        P("c"),
        P("c", rows),
        P(),
        P(rows, "c"),
        P(rows, "c"),
        P("c", rows),
        P("c"),
    )
    return jax.shard_map(
        fused, mesh=split, in_specs=placed, out_specs=P(rows, "c"), check_vma=False
    )
```

```python
import functools

import jax
import jax.numpy as jnp
from jax import lax
from jax.experimental import pallas as pl
from jax.experimental.pallas import tpu as pltpu
from jax.sharding import Mesh, PartitionSpec as P

GROUP_DIM = 128
LENGTH = 128
EPS = 1e-06
INNER = 4


def partner(at, step, count):
    if count & (count - 1) == 0:
        return at ^ step, at ^ step
    return (at + step) % count, (at - step) % count


def send(value, axis, count, step):
    pairs = [(at, partner(at, step, count)[0]) for at in range(count)]
    return lax.ppermute(value, axis, pairs)


def place(whole, piece, at, dim):
    return lax.dynamic_update_slice_in_dim(whole, piece, at * piece.shape[dim], dim)


def gather(value, axis, dim):
    count = lax.axis_size(axis)
    me = lax.axis_index(axis)
    shape = list(value.shape)
    shape[dim] *= count
    pieces = [(me, value)]
    for step in range(1, count):
        pieces.append((partner(me, step, count)[1], send(value, axis, count, step)))
    whole = jnp.zeros(shape, value.dtype)
    for at, piece in pieces:
        whole = place(whole, piece, at, dim)
    return whole


def exchange(value, axis, cut, dim):
    count = lax.axis_size(axis)
    me = lax.axis_index(axis)
    width = value.shape[cut] // count
    block = lambda at: lax.dynamic_slice_in_dim(value, at * width, width, cut)
    pieces = [(me, block(me))]
    for step in range(1, count):
        there, origin = partner(me, step, count)
        pieces.append((origin, send(block(there), axis, count, step)))
    shape = list(pieces[0][1].shape)
    shape[dim] *= count
    whole = jnp.zeros(shape, value.dtype)
    for at, piece in pieces:
        whole = place(whole, piece, at, dim)
    return whole


def scatter_sum(value, axis, dim):
    count = lax.axis_size(axis)
    me = lax.axis_index(axis)
    width = value.shape[dim] // count
    block = lambda at: lax.dynamic_slice_in_dim(value, at * width, width, dim)
    total = block(me).astype(jnp.float32)
    for step in range(1, count):
        there = partner(me, step, count)[0]
        total = total + send(block(there), axis, count, step).astype(jnp.float32)
    return total


def ring(value, axis, dim, first=None, behind=None):
    count = lax.axis_size(axis)
    me = lax.axis_index(axis)
    shape = list(value.shape)
    shape[dim] *= count
    whole = place(jnp.zeros(shape, value.dtype), value, me, dim)
    ahead = [(at, (at + 1) % count) for at in range(count)]
    back = [(at, (at - 1) % count) for at in range(count)]
    up = down = value
    for step in range(1, count // 2 + 1):
        if step == 1 and first is not None:
            up = first
        else:
            up = lax.ppermute(up, axis, ahead)
        whole = place(whole, up, (me - step) % count, dim)
        if 2 * step < count:
            if step == 1 and behind is not None:
                down = behind
            else:
                down = lax.ppermute(down, axis, back)
            whole = place(whole, down, (me + step) % count, dim)
    return whole


def half_norm(values, gain, width):
    wide = values.astype(jnp.float32)
    squares = lax.psum(jnp.sum(wide * wide, axis=1, keepdims=True), "tp")
    return wide * lax.rsqrt(squares / width + EPS) * gain


def dot(left, right):
    return jnp.dot(left, right, preferred_element_type=jnp.float32)


def local(
    tokens,
    mixer_gain,
    pool_input,
    group_weight,
    channel_scale,
    pool_output,
    ffn_gain,
    gate_weight,
    up_weight,
    down_weight,
    final_gain,
):
    tp = lax.axis_index("tp")
    columns = tokens.shape[1]
    width = columns * lax.axis_size("tp")
    inner = lax.axis_size("inner")

    full_rows = gather(tokens, "tp", 1)
    depth, hidden_all = gate_weight.shape
    hidden_width = hidden_all // inner
    both = jnp.concatenate(
        [
            gate_weight.reshape(depth, inner, hidden_width),
            up_weight.reshape(depth, inner, hidden_width),
        ],
        axis=2,
    ).reshape(depth, inner * 2 * hidden_width)
    pool_in = ring(pool_input[None, None], "outer", 0)
    pool_out = ring(pool_output[None, None], "outer", 0)
    both = exchange(both, "inner", 1, 0)
    pool_in, pool_out, both = lax.optimization_barrier((pool_in, pool_out, both))
    pool_in = gather(pool_in, "inner", 1).reshape(width, pool_input.shape[1])
    down_weight, pool_in = lax.optimization_barrier((down_weight, pool_in))
    pool_out = gather(pool_out, "inner", 1)
    pool_out = jnp.transpose(pool_out, (2, 0, 1, 3)).reshape(pool_output.shape[0], width)
    planes = lax.axis_size("outer")
    first = lax.ppermute(both, "outer", [(at, (at + 1) % planes) for at in range(planes)])
    behind = lax.ppermute(both, "outer", [(at, (at - 1) % planes) for at in range(planes)])
    down = exchange(down_weight, "inner", 0, 1)

    wide = full_rows.astype(jnp.float32)
    first_normed = (
        wide * lax.rsqrt(jnp.mean(wide * wide, axis=-1, keepdims=True) + EPS) * mixer_gain
    ).astype(jnp.bfloat16)
    row_count = first_normed.shape[0]
    pooled_in = dot(first_normed, pool_in).astype(jnp.bfloat16)
    local_groups = group_weight.shape[0]
    group_ids = tp * local_groups + jnp.arange(local_groups, dtype=jnp.int32)
    windows = jnp.left_shift(jnp.int32(2), group_ids % 4)
    later = jnp.arange(LENGTH, dtype=jnp.int32)[None, :, None]
    earlier = jnp.arange(LENGTH, dtype=jnp.int32)[None, None, :]
    reach = windows[:, None, None]
    inside = (earlier <= later) & (earlier > later - reach)
    band = inside.astype(jnp.bfloat16)
    divisor = jnp.minimum(later[:, :, 0] + 1, windows[:, None]).astype(jnp.float32)
    grid_low = pooled_in.reshape(row_count // LENGTH, LENGTH, local_groups, GROUP_DIM)
    window_sums = jnp.einsum("gts,nsgc->ntgc", band, grid_low, preferred_element_type=jnp.float32)
    average = window_sums / jnp.transpose(divisor)[None, :, :, None]
    pooled = (
        (average - grid_low.astype(jnp.float32))
        .astype(jnp.bfloat16)
        .reshape(row_count, local_groups, GROUP_DIM)
    )
    mapped = jnp.einsum("ngc,gcd->ngd", pooled, group_weight, preferred_element_type=jnp.float32)
    grouped = (mapped.reshape(row_count, local_groups * GROUP_DIM) * channel_scale).astype(
        jnp.bfloat16
    )
    mixer_terms = dot(grouped, pool_out).astype(jnp.bfloat16)
    mixer_terms, first, behind, both, down = lax.optimization_barrier(
        (mixer_terms, first, behind, both, down)
    )
    both = ring(both, "outer", 0, first, behind)
    mixer_out = scatter_sum(mixer_terms, "tp", 1)
    middle = (tokens.astype(jnp.float32) + mixer_out).astype(jnp.bfloat16)

    own_gain = lax.dynamic_slice_in_dim(ffn_gain, tp * columns, columns, 0)
    second_half = half_norm(middle, own_gain, width).astype(jnp.bfloat16)
    ahead = lax.ppermute(down, "outer", [(at, (at + 1) % planes) for at in range(planes)])
    after = lax.ppermute(down, "outer", [(at, (at - 1) % planes) for at in range(planes)])
    second_half, both, ahead, after, down = lax.optimization_barrier(
        (gather(second_half, "inner", 0), both, ahead, after, down)
    )
    down = ring(down, "outer", 1, ahead, after)
    second_normed = gather(second_half, "tp", 1)
    gate = dot(second_normed, both[:, :hidden_width])
    upward = dot(second_normed, both[:, hidden_width:])
    hidden = (jax.nn.silu(gate) * upward).astype(jnp.bfloat16)
    ffn_terms = dot(hidden, down).astype(jnp.bfloat16)
    over_cores = scatter_sum(ffn_terms, "tp", 1).astype(jnp.bfloat16)
    ffn_out = scatter_sum(over_cores, "inner", 0)
    closing = middle.astype(jnp.float32) + ffn_out
    return half_norm(closing, final_gain, width).astype(jnp.bfloat16)


def general(mesh):
    fs, tp = mesh.shape["fs"], mesh.shape["tp"]
    inner = INNER if fs % INNER == 0 else 1
    split = Mesh(mesh.devices.reshape(fs // inner, inner, tp), ("outer", "inner", "tp"))
    rows = ("outer", "inner")
    placed = (
        P(rows, "tp"),
        P(),
        P(rows, "tp"),
        P("tp", None, None),
        P("tp"),
        P("tp", rows),
        P(),
        P(rows, "tp"),
        P(rows, "tp"),
        P("tp", rows),
        P("tp"),
    )
    return jax.shard_map(
        local, mesh=split, in_specs=placed, out_specs=P(rows, "tp"), check_vma=False
    )


AXES = ("zh", "zl", "y", "x", "c")
MESH = pl.DeviceIdType.MESH
PIECES = 16
SENDS = 56
ROLE_SENDS = 24


def rel(a=0, b=0, e=0, d=0):
    return 8 * a + 4 * b + 2 * e + d


def kernel(
    tok_in,
    mixer_gain_in,
    pin,
    gw_in,
    cs_in,
    pout,
    ffn_gain_in,
    gate,
    up,
    dn,
    final_gain_in,
    out,
    OUT,
    final_gain,
    tok,
    mixer_gain,
    gw,
    cs,
    ffn_gain,
    RAW,
    gu,
    TOKR,
    FN,
    PIN,
    POUT,
    GRP,
    MT,
    MR,
    MID,
    SQS,
    SQR,
    SN,
    GU,
    DN,
    ACC,
    H,
    TS,
    TR,
    OWN,
    S1,
    R1,
    S2,
    R2,
    CL,
    send_sems,
    local_sems,
    r_pin,
    r_pout,
    r_gu,
    r_dn,
    r_misc,
    r_sn,
    r_snc,
    r_tp,
    r_s1,
    r_s2,
    r_s3,
):
    at = {name: lax.axis_index(name) for name in AXES}
    zh, zl, y, x, c = (at[name] for name in AXES)
    rows, half = tok.shape
    depth = pin.shape[0]
    hid = dn.shape[1]
    pad = H.shape[2]
    chans = pin.shape[1]
    width = 2 * half
    tile = 256

    fold = zl + zh - 2 * zl * zh

    def other(*names):
        flip = {n: n in names for n in AXES}
        flip["zl"] = flip["zl"] != flip["zh"]
        return tuple(1 - at[n] if flip[n] else at[n] for n in AXES)

    sent = []
    spare = list(range(SENDS))

    def remote(src, dst, ssem, rsem, *names):
        return pltpu.make_async_remote_copy(
            src_ref=src,
            dst_ref=dst,
            send_sem=send_sems.at[ssem],
            recv_sem=rsem,
            device_id=other(*names),
            device_id_type=MESH,
        )

    def prepare(src, dst, rsem, *names):
        ssem = spare.pop(0)
        copy = remote(src, dst, ssem, rsem, *names)
        sent.append((copy, ssem))
        return copy

    def push(src, dst, rsem, *names):
        prepare(src, dst, rsem, *names).start()

    def retire(copies):
        for copy, ssem in copies:
            copy.wait_send()
            spare.append(ssem)
        copies.clear()

    def got(dst, rsem, name):
        with jax.named_scope("wait_" + name):
            pltpu.make_async_remote_copy(
                src_ref=dst,
                dst_ref=dst,
                send_sem=send_sems.at[0],
                recv_sem=rsem,
                device_id=other("c"),
                device_id_type=MESH,
            ).wait_recv()

    def bits(a, b, e, d):
        m = b if a == 0 else 1 - b
        return (
            zh + a * (1 - 2 * zh),
            zl + m * (1 - 2 * zl),
            y + e * (1 - 2 * y),
            x + d * (1 - 2 * x),
        )

    def natural(a, b, e, d):
        h, l, v, u = bits(a, b, e, d)
        return pl.multiple_of((8 * h + 4 * l + 2 * v + u) * depth, depth)

    def grouped_at(a, b, e, d):
        h, l, v, u = bits(a, b, e, d)
        return pl.multiple_of((8 * h + 4 * v + 2 * l + u) * depth, depth)

    def pin_at(*k):
        return PIN.at[pl.ds(natural(*k), depth), :]

    def pout_at(*k):
        return POUT.at[:, pl.ds(natural(*k), depth)]

    def gu_at(*k):
        return GU.at[pl.ds(grouped_at(*k), depth), :]

    def dn_at(*k):
        return DN.at[pl.ds(0, hid), pl.ds(natural(*k), depth)]

    flips = {"zh": (1, 0, 0, 0), "zl": (0, 1, 0, 0), "y": (0, 0, 1, 0), "x": (0, 0, 0, 1)}

    def forward(place, sems, k, names, src=None):
        for name in names:
            there = tuple(1 - p if q else p for p, q in zip(k, flips[name]))
            push(place(*k) if src is None else src, place(*k), sems.at[rel(*there)], name)

    def start_if(condition, copy):
        @pl.when(condition)
        def _():
            copy.start()

    def arrive(place, sems, k):
        name = place.__name__ + "".join(str(bit) if isinstance(bit, int) else "v" for bit in k)
        got(place(*k), sems.at[rel(*k)], name)

    DN[pl.ds(hid, pad - hid), :] = jnp.zeros((pad - hid, width), DN.dtype)

    raw = [
        pltpu.make_async_copy(gate, RAW.at[0], local_sems.at[4]),
        pltpu.make_async_copy(up, RAW.at[1], local_sems.at[5]),
    ]
    for copy in raw:
        copy.start()
    ready = [
        pltpu.make_async_copy(source, target, local_sems.at[6 + n])
        for n, (source, target) in enumerate(
            (
                (tok_in, tok),
                (mixer_gain_in, mixer_gain),
                (gw_in, gw),
                (cs_in, cs),
                (ffn_gain_in, ffn_gain),
                (final_gain_in, final_gain),
            )
        )
    ]

    barrier = pltpu.get_barrier_semaphore()
    peers = (("c",), ("x",), ("y",), ("zl",), ("zh",), ("zl", "x"))
    for names in peers:
        pl.semaphore_signal(barrier, inc=1, device_id=other(*names), device_id_type=MESH)
    with jax.named_scope("barrier"):
        pl.semaphore_wait(barrier, len(peers))

    mine = (0, 0, 0, 0)
    quarter = 2 * fold + x
    push(tok_in, TOKR, r_misc.at[0], "c")
    forward(pin_at, r_pin, mine, ("zh", "zl", "x", "y"), pin)
    forward(pout_at, r_pout, mine, ("zh", "zl", "y", "x"), pout)
    locals_ = [
        pltpu.make_async_copy(pin, pin_at(*mine), local_sems.at[0]),
        pltpu.make_async_copy(pout, pout_at(*mine), local_sems.at[1]),
        pltpu.make_async_copy(dn.at[quarter], dn_at(*mine), local_sems.at[3]),
    ]
    for copy in locals_ + ready:
        copy.start()

    for copy in raw:
        copy.wait()
    lanes = GROUP_DIM
    low_lane = lax.broadcasted_iota(jnp.int32, (16, lanes), 1) < lanes // 2
    full = hid // lanes

    @pl.loop(0, depth // 16)
    def _(i):
        at_rows = pl.ds(pl.multiple_of(i * 16, 16), 16)
        own_rows = pl.ds(pl.multiple_of(grouped_at(*mine) + i * 16, 16), 16)

        def block(which, m):
            return RAW[which, at_rows, m * lanes : (m + 1) * lanes].astype(jnp.float32)

        def turned(which, m):
            return pltpu.roll(block(which, m), lanes // 2, 1)

        for q in range(4):
            first, skew = divmod(q * hid, lanes)
            for which in range(2):
                for j in range(full):
                    m = first + j
                    if skew == 0:
                        value = block(which, m)
                    else:
                        value = jnp.where(low_lane, turned(which, m), turned(which, m + 1))
                    start = (2 * j + which) * lanes
                    gu[q, at_rows, start : start + lanes] = value.astype(gu.dtype)
            m = first + full
            if skew == 0:
                value = jnp.where(low_lane, block(0, m), turned(1, m))
            else:
                value = jnp.where(low_lane, turned(0, m), block(1, m))
            gu[q, at_rows, 2 * full * lanes :] = value.astype(gu.dtype)
        GU[own_rows, :] = gu[quarter, at_rows, :]

    own_over = prepare(gu.at[quarter], gu_at(*mine), r_gu.at[rel(a=1)], "zh")
    start_if(fold == 1, own_over)

    trades = (((0, 0, 0, 1), ("x",)), ((0, 1, 0, 0), ("zl",)), ((0, 1, 0, 1), ("zl", "x")))

    def trade(place, sems, source, which):
        k, names = which
        _, b, _, d = k
        there = 2 * (1 - fold if b else fold) + (1 - x if d else x)
        push(source.at[there], place(*mine), sems.at[rel(*k)], *names)

    def low(l, a=0):
        return zl if l == a else 1 - zl

    def side(u):
        return x if u == 0 else 1 - x

    chunk = 32

    def normalize():
        got(TOKR, r_misc.at[0], "tok")
        for copy in ready:
            copy.wait()

        @pl.loop(0, rows // chunk)
        def _(i):
            at_rows = pl.ds(pl.multiple_of(i * chunk, chunk), chunk)
            a = tok[at_rows, :].astype(jnp.float32)
            b = TOKR[at_rows, :].astype(jnp.float32)
            mean = (
                jnp.sum(a * a, axis=1, keepdims=True) + jnp.sum(b * b, axis=1, keepdims=True)
            ) / width
            scale = lax.rsqrt(mean + EPS)
            FN[0, at_rows, :] = (a * scale * mixer_gain[c]).astype(FN.dtype)
            FN[1, at_rows, :] = (b * scale * mixer_gain[1 - c]).astype(FN.dtype)

    def across(a, b):
        arrive(pin_at, r_pin, (a, b, 0, 1))
        forward(pin_at, r_pin, (a, b, 0, 1), ("y",))
        arrive(pout_at, r_pout, (a, b, 1, 0))
        forward(pout_at, r_pout, (a, b, 1, 0), ("x",))

    across(0, 0)
    arrive(pin_at, r_pin, (1, 0, 0, 0))
    forward(pin_at, r_pin, (1, 0, 0, 0), ("zl", "x", "y"))
    arrive(pout_at, r_pout, (1, 0, 0, 0))
    forward(pout_at, r_pout, (1, 0, 0, 0), ("zl", "y", "x"))
    for k in ((0, 1, 0, 0), (1, 1, 0, 0)):
        arrive(pin_at, r_pin, k)
        forward(pin_at, r_pin, k, ("x", "y"))
        arrive(pout_at, r_pout, k)
        forward(pout_at, r_pout, k, ("y", "x"))
    trade(gu_at, r_gu, gu, trades[1])
    start_if(fold == 0, own_over)
    normalize()
    for a, b in ((1, 0), (0, 1), (1, 1)):
        across(a, b)
    forward(gu_at, r_gu, mine, ("y",), gu.at[quarter])

    def pool_part(v, n):
        total = None
        for e in range(2):
            which = c + e * (1 - 2 * c)
            for l in range(2):
                columns = pl.multiple_of((4 * l + 2 * v) * depth, 2 * depth)
                at_pin = pl.multiple_of(which * half + columns, 2 * depth)
                term = dot(
                    FN[e, :, pl.ds(columns, 2 * depth)],
                    PIN[pl.ds(at_pin, 2 * depth), n * tile : (n + 1) * tile],
                )
                total = term if total is None else total + term
        return total

    locals_[0].wait()
    for n in range(chans // tile):
        OWN[0, n] = pool_part(y, n)

    arrive(gu_at, r_gu, trades[1][0])
    forward(gu_at, r_gu, trades[1][0], ("zh", "y"))

    for a, b in ((0, 0), (1, 0), (0, 1), (1, 1)):
        for d in range(2):
            arrive(pin_at, r_pin, (a, b, 1, d))
    trade(gu_at, r_gu, gu, trades[0])
    trade(gu_at, r_gu, gu, trades[2])
    trade(dn_at, r_dn, dn, trades[1])

    groups = gw.shape[0]
    per_tile = tile // GROUP_DIM

    later = lax.broadcasted_iota(jnp.int32, (LENGTH, LENGTH), 0)
    earlier = lax.broadcasted_iota(jnp.int32, (LENGTH, LENGTH), 1)
    place_in = lax.broadcasted_iota(jnp.int32, (LENGTH, GROUP_DIM), 0)
    for n in range(chans // tile):
        pooled_in = (OWN[0, n] + pool_part(1 - y, n)).astype(jnp.bfloat16)
        for j in range(per_tile):
            g = n * per_tile + j
            window = 2 << (g % 4)
            band = ((earlier <= later) & (earlier > later - window)).astype(jnp.float32)
            band = band.astype(jnp.bfloat16)
            divisor = jnp.minimum(place_in + 1, window).astype(jnp.float32)
            for s in range(rows // LENGTH):
                grid = pooled_in[s * LENGTH : (s + 1) * LENGTH, j * GROUP_DIM : (j + 1) * GROUP_DIM]
                average = dot(band, grid) / divisor
                pooled = (average - grid.astype(jnp.float32)).astype(jnp.bfloat16)
                mapped = dot(pooled, gw[g])
                GRP[pl.ds(s * LENGTH, LENGTH), pl.ds(g * GROUP_DIM, GROUP_DIM)] = (
                    mapped * cs[:, g * GROUP_DIM : (g + 1) * GROUP_DIM]
                ).astype(GRP.dtype)

    locals_[1].wait()
    for a, b in ((0, 0), (1, 0), (0, 1), (1, 1)):
        for e in range(2):
            arrive(pout_at, r_pout, (a, b, e, 1))

    def cols_of(which, n):
        return pl.ds(pl.multiple_of(which * half + n * tile, tile), tile)

    @pl.loop(0, half // tile)
    def _(n):
        part = dot(GRP[...], POUT[:, cols_of(1 - c, n)])
        MT[:, cols_of(0, n)] = part.astype(MT.dtype)

    pool_sent = sent[:]
    sent.clear()
    push(MT, MR, r_misc.at[1], "c")

    @pl.loop(0, half // tile)
    def _(n):
        part = dot(GRP[...], POUT[:, cols_of(c, n)])
        MID[:, cols_of(0, n)] = part.astype(MID.dtype)

    arrive(gu_at, r_gu, (1, 0, 0, 0))
    forward(gu_at, r_gu, (1, 0, 0, 0), ("y",))
    got(MR, r_misc.at[1], "mix")

    @pl.loop(0, rows // chunk)
    def _(i):
        at_rows = pl.ds(pl.multiple_of(i * chunk, chunk), chunk)
        mixed = MID[at_rows, :].astype(jnp.float32) + MR[at_rows, :].astype(jnp.float32)
        middle = (tok[at_rows, :].astype(jnp.float32) + mixed).astype(jnp.bfloat16)
        MID[at_rows, :] = middle
        wide = middle.astype(jnp.float32)
        squares = jnp.sum(wide * wide, axis=1, keepdims=True)
        SQS[0, at_rows, :] = jnp.broadcast_to(squares, (chunk, SQS.shape[2]))

    push(SQS.at[0], SQR.at[0], r_misc.at[2], "c")
    got(SQR.at[0], r_misc.at[2], "sq0")

    @pl.loop(0, rows // chunk)
    def _(i):
        at_rows = pl.ds(pl.multiple_of(i * chunk, chunk), chunk)
        squares = SQS[0, at_rows, 0:1] + SQR[0, at_rows, 0:1]
        scale = lax.rsqrt(squares / width + EPS)
        wide = MID[at_rows, :].astype(jnp.float32)
        normed = (wide * scale * ffn_gain[c]).astype(SN.dtype)
        for l in range(2):
            for v in range(2):
                source = (4 * l + 2 * v) * depth
                target = (4 * v + 2 * l) * depth
                SN[0, 0, at_rows, pl.ds(target, 2 * depth)] = normed[:, source : source + 2 * depth]

    push(SN.at[0, 0], SN.at[2, 0], r_sn.at[2], "zl")
    push(SN.at[0, 0], SN.at[1, 0], r_sn.at[1], "x")
    push(SN.at[0, 0], SN.at[0, 1], r_snc.at[0], "c")

    trade(dn_at, r_dn, dn, trades[0])
    trade(dn_at, r_dn, dn, trades[2])
    for i in (0, 2):
        arrive(gu_at, r_gu, trades[i][0])
        forward(gu_at, r_gu, trades[i][0], ("zh", "y"))
    arrive(gu_at, r_gu, (1, 1, 0, 0))
    forward(gu_at, r_gu, (1, 1, 0, 0), ("y",))
    with jax.named_scope("retire"):
        retire(pool_sent)
    got(SN.at[1, 0], r_sn.at[1], "sn1")
    push(SN.at[1, 0], SN.at[1, 1], r_snc.at[1], "c")
    got(SN.at[2, 0], r_sn.at[2], "sn2")
    push(SN.at[2, 0], SN.at[3, 0], r_sn.at[3], "x")
    push(SN.at[2, 0], SN.at[2, 1], r_snc.at[2], "c")
    locals_[2].wait()
    for which in trades:
        arrive(dn_at, r_dn, which[0])
    for l in range(2):
        for u in range(2):
            forward(dn_at, r_dn, (0, low(l), 0, side(u)), ("zh",))

    whole_tiles = GU.shape[1] // tile
    half_tile = tile // 2
    lane = lax.broadcasted_iota(jnp.int32, (rows, half_tile), 1)
    near = jnp.where(zh == c, 0, 1)
    near_rows = pl.ds(pl.multiple_of(zh * half, half), half)
    far_rows = pl.ds(pl.multiple_of((1 - zh) * half, half), half)
    last = pl.ds(whole_tiles * tile, half_tile)

    def tile_at(j, size):
        return pl.ds(pl.multiple_of(j * size, size), size)

    def begin(r):
        got(SN.at[r, 1], r_snc.at[r], f"snc{r}")
        with jax.named_scope(f"begin{r}"):

            @pl.loop(0, whole_tiles)
            def _(j):
                ACC[r, :, tile_at(j, tile)] = dot(SN[r, near], GU[near_rows, tile_at(j, tile)])

            ACC[r, :, last] = dot(SN[r, near], GU[near_rows, last])

    def gated(r):
        with jax.named_scope(f"gated{r}"):

            @pl.loop(0, whole_tiles)
            def _(j):
                both = dot(SN[r, 1 - near], GU[far_rows, tile_at(j, tile)])
                both = both + ACC[r, :, tile_at(j, tile)]
                gate, up = both[:, :half_tile], both[:, half_tile:]
                value = gate / (1.0 + jnp.exp(-gate)) * up
                H[r, :, tile_at(j, half_tile)] = value.astype(H.dtype)

            both = dot(SN[r, 1 - near], GU[far_rows, last]) + ACC[r, :, last]
            up = pltpu.roll(both, half_tile // 2, 1)
            value = both / (1.0 + jnp.exp(-both)) * up
            H[r, :, pl.ds(whole_tiles * half_tile, half_tile)] = jnp.where(
                lane < half_tile // 2, value, 0.0
            ).astype(H.dtype)

    for b, d in ((0, 0), (0, 1), (1, 0), (1, 1)):
        arrive(gu_at, r_gu, (0, b, 1, d))
    begin(0)
    arrive(gu_at, r_gu, (1, 0, 0, 1))
    forward(gu_at, r_gu, (1, 0, 0, 1), ("y",))
    begin(1)
    begin(2)
    arrive(gu_at, r_gu, (1, 1, 0, 1))
    forward(gu_at, r_gu, (1, 1, 0, 1), ("y",))
    got(SN.at[3, 0], r_sn.at[3], "sn3")
    push(SN.at[3, 0], SN.at[3, 1], r_snc.at[3], "c")
    begin(3)
    for l in range(2):
        for u in range(2):
            forward(dn_at, r_dn, (0, low(l), 0, side(u)), ("y",))
    for b, d in ((0, 0), (0, 1), (1, 0), (1, 1)):
        arrive(gu_at, r_gu, (1, b, 1, d))
    whole_steps = [(a, e, l, None) for a in range(2) for e in range(2) for l in range(2)]
    steps = whole_steps[:-1] + [whole_steps[-1][:3] + (u,) for u in range(2)]
    firsts = ("x", "zl")
    owners = (zh == c, zh != c)
    role_sent = ([], [])

    def role_copy(which, *args):
        src, dst, rsem, *names = args
        copy = remote(src, dst, SENDS + len(role_sent[which]), rsem, *names)
        role_sent[which].append(copy)
        return copy

    def place_of(s):
        a, _, _, u = steps[s]
        slot = min(s - 4 * a, 3)
        start, size = (0, tile) if u is None else (u * half_tile, half_tile)
        return a, slot, s - 4 * a, pl.ds(start, size)

    def step_cols(s, which=0):
        _, e, l, u = steps[s]
        v = y + e * (1 - 2 * y)
        start, size = (0, tile) if u is None else (u * half_tile, half_tile)
        return pl.ds(pl.multiple_of(which * half + (2 * l + v) * tile + start, size), size)

    def produce(s, blocks=(0, 1, 2, 3)):
        a, t, i, part = place_of(s)
        columns = step_cols(s, zh + a * (1 - 2 * zh))
        single = s >= 2
        if single:
            ways = [(TS.at[t, :, :, part], TR.at[t, :, :, part], r_tp.at[tp_index(s)])]
        else:
            ways = [(TS.at[t, r], TR.at[t, r], r_tp.at[tp_index(s) + r]) for r in blocks]
        overs = [role_copy(1 - a, *way, "c") for way in ways]

        @pl.when(owners[1 - a])
        def _():
            for n, r in enumerate(blocks):
                TS[t, r, :, part] = dot(H[r], DN[:, columns]).astype(TS.dtype)
                if not single:
                    overs[n].start()
            if single:
                overs[0].start()

        @pl.when(owners[a])
        def _():
            for r in blocks:
                OWN[t, r, :, part] = dot(H[r], DN[:, columns])

    def tp_index(s):
        a, t, i, part = place_of(s)
        return i if a else (4 * s if s < 2 else 6 + s)

    def crossed(s):
        a, t, i, part = place_of(s)
        got(TR.at[t, :, :, part], r_tp.at[tp_index(s)], f"tp{s}")

    def both_cores(s, r):
        a, t, i, part = place_of(s)
        if s < 2:
            got(TR.at[t, r], r_tp.at[tp_index(s) + r], f"tp{s}r{r}")
        return OWN[t, r, :, part] + TR[t, r, :, part].astype(jnp.float32)

    def halves_of(axis):
        return ((1, 3), (0, 2)) if axis == "x" else ((2, 3), (0, 1))

    def first_stage(s):
        a, t, i, part = place_of(s)
        axis = firsts[s % 2]
        over = role_copy(a, S1.at[t], R1.at[t], r_s1.at[i], axis)

        @pl.when(owners[a])
        def _():
            if s >= 2:
                crossed(s)
            for n, r in enumerate(halves_of(axis)[0]):
                S1[t, n] = both_cores(s, r).astype(S1.dtype)
            over.start()

    def second_stage(s):
        a, t, i, part = place_of(s)
        over = role_copy(a, S2.at[t], R2.at[t], r_s2.at[i], firsts[1 - s % 2])
        keep, give = halves_of(firsts[s % 2])[1]

        @pl.when(owners[a])
        def _():
            given = both_cores(s, give)
            got(R1.at[t], r_s1.at[i], f"first{s}")
            S2[t] = (given + R1[t, 1].astype(jnp.float32)).astype(S2.dtype)
            over.start()
            CL[t] = both_cores(s, keep) + R1[t, 0].astype(jnp.float32)

    def close(s, t, part, columns, summed):
        closing = MID[:, columns].astype(jnp.float32) + summed
        CL[t, :, part] = closing
        squares = jnp.sum(closing * closing, axis=1, keepdims=True)
        squares = jnp.broadcast_to(squares, SQS.shape[1:])
        SQS[1] = squares if t == 0 else SQS[1] + squares

    def finish(s):
        a, t, i, part = place_of(s)
        columns = step_cols(s)

        @pl.when(owners[a])
        def _():
            got(R2.at[t], r_s2.at[i], f"second{s}")
            close(s, t, part, columns, CL[t] + R2[t].astype(jnp.float32))

    def straight(t, part):
        return (
            (3, S2.at[t, :, part], R2.at[t, :, part], r_s2, ("zl", "x")),
            (1, S1.at[t, 0, :, part], R1.at[t, 0, :, part], r_s1, ("x",)),
            (2, S1.at[t, 1, :, part], R1.at[t, 1, :, part], r_s3, ("zl",)),
        )

    def scatter(s):
        a, t, i, part = place_of(s)
        ways = straight(t, part)
        overs = [
            role_copy(a, source, target, sems.at[i], *names)
            for _, source, target, sems, names in ways
        ]

        @pl.when(owners[a])
        def _():
            crossed(s)
            for (r, source, _, _, _), over in zip(ways, overs):
                source[...] = both_cores(s, r).astype(S1.dtype)
                over.start()
            CL[t, :, part] = both_cores(s, 0)

    def gather_sums(s):
        a, t, i, part = place_of(s)
        columns = step_cols(s)

        @pl.when(owners[a])
        def _():
            summed = CL[t, :, part]
            for r, _, target, sems, _ in straight(t, part):
                got(target, sems.at[i], f"sum{s}from{r}")
                summed = summed + target[...].astype(jnp.float32)
            close(s, t, part, columns, summed)

    def relay(l):
        for u in range(2):
            k = (1, low(l, 1), 0, side(u))
            arrive(dn_at, r_dn, k)
            forward(dn_at, r_dn, k, ("y",))

    def landed(a, l, which=(0, 1)):
        for u in which:
            arrive(dn_at, r_dn, (a, low(l, a), 1, side(u)))

    gated(3)
    gated(1)
    produce(0, (1, 3))
    gated(2)
    produce(1, (2, 3))
    first_stage(0)
    gated(0)
    produce(0, (0, 2))
    produce(1, (0, 1))
    first_stage(1)
    relay(0)
    produce(4)
    landed(0, 0)
    produce(2)
    landed(0, 1)
    produce(3)
    second_stage(0)
    second_stage(1)
    first_stage(2)
    first_stage(3)
    first_stage(4)
    relay(1)
    produce(5)
    first_stage(5)
    landed(1, 0)
    produce(6)
    first_stage(6)
    second_stage(4)
    landed(1, 1, (0,))
    produce(7)
    scatter(7)
    for s in (2, 3, 5):
        second_stage(s)
    landed(1, 1, (1,))
    produce(8)
    scatter(8)
    second_stage(6)
    for s in range(7):
        finish(s)
    for s in (7, 8):
        gather_sums(s)
    push(SQS.at[1], SQR.at[1], r_misc.at[3], "c")
    got(SQR.at[1], r_misc.at[3], "sq1")
    scale = lax.rsqrt((SQS[1, :, 0:1] + SQR[1, :, 0:1]) / width + EPS)
    finals = []
    for t in range(4):
        columns = step_cols(t)
        OUT[:, columns] = (CL[t] * scale * final_gain[:, columns]).astype(out.dtype)
        copy = pltpu.make_async_copy(
            OUT.at[:, columns], out.at[:, columns], local_sems.at[12 + t]
        )
        copy.start()
        finals.append(copy)

    with jax.named_scope("drain"):
        retire(sent)
        for which in range(2):

            @pl.when(owners[which])
            def _():
                for copy in role_sent[which]:
                    copy.wait_send()

        for copy in finals:
            copy.wait()


def fused(
    tokens,
    mixer_gain,
    pool_input,
    group_weight,
    channel_scale,
    pool_output,
    ffn_gain,
    gate_weight,
    up_weight,
    down_weight,
    final_gain,
):
    rows, half = tokens.shape
    depth, hidden_all = gate_weight.shape
    hid = hidden_all // 4
    full = hid // GROUP_DIM
    chans = pool_input.shape[1]
    dn = down_weight.reshape(4, hid, depth)
    pad = (full + 1) * GROUP_DIM
    bf, f32 = jnp.bfloat16, jnp.float32
    hbm = pl.BlockSpec(memory_space=pl.ANY)
    dma = pltpu.SemaphoreType.DMA
    tile = 256
    scratch = [
        pltpu.VMEM((rows, half), bf),
        pltpu.VMEM((1, half), f32),
        pltpu.VMEM((rows, half), bf),
        pltpu.VMEM((2, 1, half), f32),
        pltpu.VMEM(group_weight.shape, bf),
        pltpu.VMEM((1, chans), f32),
        pltpu.VMEM((2, 1, half), f32),
        pltpu.VMEM((2, depth, hidden_all), bf),
        pltpu.VMEM((4, depth, 2 * hid), bf),
        pltpu.VMEM((rows, half), bf),
        pltpu.VMEM((2, rows, half), bf),
        pltpu.VMEM((2 * half, chans), bf),
        pltpu.VMEM((chans, 2 * half), bf),
        pltpu.VMEM((rows, chans), bf),
        pltpu.VMEM((rows, half), bf),
        pltpu.VMEM((rows, half), bf),
        pltpu.VMEM((rows, half), bf),
        pltpu.VMEM((2, rows, GROUP_DIM), f32),
        pltpu.VMEM((2, rows, GROUP_DIM), f32),
        pltpu.VMEM((4, 2, rows, half), bf),
        pltpu.VMEM((2 * half, 2 * hid), bf),
        pltpu.VMEM((pad, 2 * half), bf),
        pltpu.VMEM((4, rows, 2 * hid), f32),
        pltpu.VMEM((4, rows, pad), bf),
        pltpu.VMEM((4, 4, rows, tile), bf),
        pltpu.VMEM((4, 4, rows, tile), bf),
        pltpu.VMEM((4, 4, rows, tile), f32),
        pltpu.VMEM((4, 2, rows, tile), bf),
        pltpu.VMEM((4, 2, rows, tile), bf),
        pltpu.VMEM((4, rows, tile), bf),
        pltpu.VMEM((4, rows, tile), bf),
        pltpu.VMEM((4, rows, tile), f32),
        dma((SENDS + ROLE_SENDS,)),
        dma((16,)),
        dma((PIECES,)),
        dma((PIECES,)),
        dma((PIECES,)),
        dma((PIECES,)),
        dma((4,)),
        dma((4,)),
        dma((4,)),
        dma((10,)),
        dma((5,)),
        dma((5,)),
        dma((5,)),
    ]
    return pl.pallas_call(
        kernel,
        out_shape=jax.ShapeDtypeStruct((rows, half), bf),
        in_specs=[hbm] * 11,
        out_specs=hbm,
        scratch_shapes=scratch,
        compiler_params=pltpu.CompilerParams(
            collective_id=0, has_side_effects=True, vmem_limit_bytes=67043328
        ),
    )(
        tokens,
        mixer_gain.reshape(2, 1, half),
        pool_input,
        group_weight,
        channel_scale.reshape(1, chans),
        pool_output,
        ffn_gain.reshape(2, 1, half),
        gate_weight,
        up_weight,
        dn,
        final_gain.reshape(1, half),
    )


def solution(mesh):
    fs, tp = mesh.shape["fs"], mesh.shape["tp"]
    if fs != PIECES or tp != 2:
        return general(mesh)
    split = Mesh(mesh.devices.reshape(2, 2, 2, 2, 2), AXES)
    rows = AXES[:4]
    placed = (
        P(rows, "c"),
        P(),
        P(rows, "c"),
        P("c", None, None),
        P("c"),
        P("c", rows),
        P(),
        P(rows, "c"),
        P(rows, "c"),
        P("c", rows),
        P("c"),
    )
    return jax.shard_map(
        fused, mesh=split, in_specs=placed, out_specs=P(rows, "c"), check_vma=False
    )
```

```python
import functools

import jax
import jax.numpy as jnp
from jax import lax
from jax.experimental import pallas as pl
from jax.experimental.pallas import tpu as pltpu
from jax.sharding import Mesh, PartitionSpec as P

GROUP_DIM = 128
LENGTH = 128
EPS = 1e-06
INNER = 4


def partner(at, step, count):
    if count & (count - 1) == 0:
        return at ^ step, at ^ step
    return (at + step) % count, (at - step) % count


def send(value, axis, count, step):
    pairs = [(at, partner(at, step, count)[0]) for at in range(count)]
    return lax.ppermute(value, axis, pairs)


def place(whole, piece, at, dim):
    return lax.dynamic_update_slice_in_dim(whole, piece, at * piece.shape[dim], dim)


def gather(value, axis, dim):
    count = lax.axis_size(axis)
    me = lax.axis_index(axis)
    shape = list(value.shape)
    shape[dim] *= count
    pieces = [(me, value)]
    for step in range(1, count):
        pieces.append((partner(me, step, count)[1], send(value, axis, count, step)))
    whole = jnp.zeros(shape, value.dtype)
    for at, piece in pieces:
        whole = place(whole, piece, at, dim)
    return whole


def exchange(value, axis, cut, dim):
    count = lax.axis_size(axis)
    me = lax.axis_index(axis)
    width = value.shape[cut] // count
    block = lambda at: lax.dynamic_slice_in_dim(value, at * width, width, cut)
    pieces = [(me, block(me))]
    for step in range(1, count):
        there, origin = partner(me, step, count)
        pieces.append((origin, send(block(there), axis, count, step)))
    shape = list(pieces[0][1].shape)
    shape[dim] *= count
    whole = jnp.zeros(shape, value.dtype)
    for at, piece in pieces:
        whole = place(whole, piece, at, dim)
    return whole


def scatter_sum(value, axis, dim):
    count = lax.axis_size(axis)
    me = lax.axis_index(axis)
    width = value.shape[dim] // count
    block = lambda at: lax.dynamic_slice_in_dim(value, at * width, width, dim)
    total = block(me).astype(jnp.float32)
    for step in range(1, count):
        there = partner(me, step, count)[0]
        total = total + send(block(there), axis, count, step).astype(jnp.float32)
    return total


def ring(value, axis, dim, first=None, behind=None):
    count = lax.axis_size(axis)
    me = lax.axis_index(axis)
    shape = list(value.shape)
    shape[dim] *= count
    whole = place(jnp.zeros(shape, value.dtype), value, me, dim)
    ahead = [(at, (at + 1) % count) for at in range(count)]
    back = [(at, (at - 1) % count) for at in range(count)]
    up = down = value
    for step in range(1, count // 2 + 1):
        if step == 1 and first is not None:
            up = first
        else:
            up = lax.ppermute(up, axis, ahead)
        whole = place(whole, up, (me - step) % count, dim)
        if 2 * step < count:
            if step == 1 and behind is not None:
                down = behind
            else:
                down = lax.ppermute(down, axis, back)
            whole = place(whole, down, (me + step) % count, dim)
    return whole


def half_norm(values, gain, width):
    wide = values.astype(jnp.float32)
    squares = lax.psum(jnp.sum(wide * wide, axis=1, keepdims=True), "tp")
    return wide * lax.rsqrt(squares / width + EPS) * gain


def dot(left, right):
    return jnp.dot(left, right, preferred_element_type=jnp.float32)


def local(
    tokens,
    mixer_gain,
    pool_input,
    group_weight,
    channel_scale,
    pool_output,
    ffn_gain,
    gate_weight,
    up_weight,
    down_weight,
    final_gain,
):
    tp = lax.axis_index("tp")
    columns = tokens.shape[1]
    width = columns * lax.axis_size("tp")
    inner = lax.axis_size("inner")

    full_rows = gather(tokens, "tp", 1)
    depth, hidden_all = gate_weight.shape
    hidden_width = hidden_all // inner
    both = jnp.concatenate(
        [
            gate_weight.reshape(depth, inner, hidden_width),
            up_weight.reshape(depth, inner, hidden_width),
        ],
        axis=2,
    ).reshape(depth, inner * 2 * hidden_width)
    pool_in = ring(pool_input[None, None], "outer", 0)
    pool_out = ring(pool_output[None, None], "outer", 0)
    both = exchange(both, "inner", 1, 0)
    pool_in, pool_out, both = lax.optimization_barrier((pool_in, pool_out, both))
    pool_in = gather(pool_in, "inner", 1).reshape(width, pool_input.shape[1])
    down_weight, pool_in = lax.optimization_barrier((down_weight, pool_in))
    pool_out = gather(pool_out, "inner", 1)
    pool_out = jnp.transpose(pool_out, (2, 0, 1, 3)).reshape(pool_output.shape[0], width)
    planes = lax.axis_size("outer")
    first = lax.ppermute(both, "outer", [(at, (at + 1) % planes) for at in range(planes)])
    behind = lax.ppermute(both, "outer", [(at, (at - 1) % planes) for at in range(planes)])
    down = exchange(down_weight, "inner", 0, 1)

    wide = full_rows.astype(jnp.float32)
    first_normed = (
        wide * lax.rsqrt(jnp.mean(wide * wide, axis=-1, keepdims=True) + EPS) * mixer_gain
    ).astype(jnp.bfloat16)
    row_count = first_normed.shape[0]
    pooled_in = dot(first_normed, pool_in).astype(jnp.bfloat16)
    local_groups = group_weight.shape[0]
    group_ids = tp * local_groups + jnp.arange(local_groups, dtype=jnp.int32)
    windows = jnp.left_shift(jnp.int32(2), group_ids % 4)
    later = jnp.arange(LENGTH, dtype=jnp.int32)[None, :, None]
    earlier = jnp.arange(LENGTH, dtype=jnp.int32)[None, None, :]
    reach = windows[:, None, None]
    inside = (earlier <= later) & (earlier > later - reach)
    band = inside.astype(jnp.bfloat16)
    divisor = jnp.minimum(later[:, :, 0] + 1, windows[:, None]).astype(jnp.float32)
    grid_low = pooled_in.reshape(row_count // LENGTH, LENGTH, local_groups, GROUP_DIM)
    window_sums = jnp.einsum("gts,nsgc->ntgc", band, grid_low, preferred_element_type=jnp.float32)
    average = window_sums / jnp.transpose(divisor)[None, :, :, None]
    pooled = (
        (average - grid_low.astype(jnp.float32))
        .astype(jnp.bfloat16)
        .reshape(row_count, local_groups, GROUP_DIM)
    )
    mapped = jnp.einsum("ngc,gcd->ngd", pooled, group_weight, preferred_element_type=jnp.float32)
    grouped = (mapped.reshape(row_count, local_groups * GROUP_DIM) * channel_scale).astype(
        jnp.bfloat16
    )
    mixer_terms = dot(grouped, pool_out).astype(jnp.bfloat16)
    mixer_terms, first, behind, both, down = lax.optimization_barrier(
        (mixer_terms, first, behind, both, down)
    )
    both = ring(both, "outer", 0, first, behind)
    mixer_out = scatter_sum(mixer_terms, "tp", 1)
    middle = (tokens.astype(jnp.float32) + mixer_out).astype(jnp.bfloat16)

    own_gain = lax.dynamic_slice_in_dim(ffn_gain, tp * columns, columns, 0)
    second_half = half_norm(middle, own_gain, width).astype(jnp.bfloat16)
    ahead = lax.ppermute(down, "outer", [(at, (at + 1) % planes) for at in range(planes)])
    after = lax.ppermute(down, "outer", [(at, (at - 1) % planes) for at in range(planes)])
    second_half, both, ahead, after, down = lax.optimization_barrier(
        (gather(second_half, "inner", 0), both, ahead, after, down)
    )
    down = ring(down, "outer", 1, ahead, after)
    second_normed = gather(second_half, "tp", 1)
    gate = dot(second_normed, both[:, :hidden_width])
    upward = dot(second_normed, both[:, hidden_width:])
    hidden = (jax.nn.silu(gate) * upward).astype(jnp.bfloat16)
    ffn_terms = dot(hidden, down).astype(jnp.bfloat16)
    over_cores = scatter_sum(ffn_terms, "tp", 1).astype(jnp.bfloat16)
    ffn_out = scatter_sum(over_cores, "inner", 0)
    closing = middle.astype(jnp.float32) + ffn_out
    return half_norm(closing, final_gain, width).astype(jnp.bfloat16)


def general(mesh):
    fs, tp = mesh.shape["fs"], mesh.shape["tp"]
    inner = INNER if fs % INNER == 0 else 1
    split = Mesh(mesh.devices.reshape(fs // inner, inner, tp), ("outer", "inner", "tp"))
    rows = ("outer", "inner")
    placed = (
        P(rows, "tp"),
        P(),
        P(rows, "tp"),
        P("tp", None, None),
        P("tp"),
        P("tp", rows),
        P(),
        P(rows, "tp"),
        P(rows, "tp"),
        P("tp", rows),
        P("tp"),
    )
    return jax.shard_map(
        local, mesh=split, in_specs=placed, out_specs=P(rows, "tp"), check_vma=False
    )


AXES = ("zh", "zl", "y", "x", "c")
MESH = pl.DeviceIdType.MESH
PIECES = 16
SENDS = 56
ROLE_SENDS = 24


def rel(a=0, b=0, e=0, d=0):
    return 8 * a + 4 * b + 2 * e + d


def kernel(
    tok_in,
    mixer_gain_in,
    pin,
    gw_in,
    cs_in,
    pout,
    ffn_gain_in,
    gate,
    up,
    dn,
    final_gain_in,
    out,
    OUT,
    final_gain,
    tok,
    mixer_gain,
    gw,
    cs,
    ffn_gain,
    RAW,
    gu,
    TOKR,
    FN,
    PIN,
    POUT,
    GRP,
    MT,
    MR,
    MID,
    SQS,
    SQR,
    SN,
    GU,
    DN,
    ACC,
    H,
    TS,
    TR,
    OWN,
    S1,
    R1,
    S2,
    R2,
    CL,
    send_sems,
    local_sems,
    r_pin,
    r_pout,
    r_gu,
    r_dn,
    r_misc,
    r_sn,
    r_snc,
    r_tp,
    r_s1,
    r_s2,
    r_s3,
):
    at = {name: lax.axis_index(name) for name in AXES}
    zh, zl, y, x, c = (at[name] for name in AXES)
    rows, half = tok.shape
    depth = pin.shape[0]
    hid = dn.shape[1]
    pad = H.shape[2]
    chans = pin.shape[1]
    width = 2 * half
    tile = 256

    fold = zl + zh - 2 * zl * zh

    def other(*names):
        flip = {n: n in names for n in AXES}
        flip["zl"] = flip["zl"] != flip["zh"]
        return tuple(1 - at[n] if flip[n] else at[n] for n in AXES)

    sent = []
    spare = list(range(SENDS))

    def remote(src, dst, ssem, rsem, *names):
        return pltpu.make_async_remote_copy(
            src_ref=src,
            dst_ref=dst,
            send_sem=send_sems.at[ssem],
            recv_sem=rsem,
            device_id=other(*names),
            device_id_type=MESH,
        )

    def prepare(src, dst, rsem, *names):
        ssem = spare.pop(0)
        copy = remote(src, dst, ssem, rsem, *names)
        sent.append((copy, ssem))
        return copy

    def push(src, dst, rsem, *names):
        prepare(src, dst, rsem, *names).start()

    def retire(copies):
        for copy, ssem in copies:
            copy.wait_send()
            spare.append(ssem)
        copies.clear()

    def got(dst, rsem, name):
        with jax.named_scope("wait_" + name):
            pltpu.make_async_remote_copy(
                src_ref=dst,
                dst_ref=dst,
                send_sem=send_sems.at[0],
                recv_sem=rsem,
                device_id=other("c"),
                device_id_type=MESH,
            ).wait_recv()

    def bits(a, b, e, d):
        m = b if a == 0 else 1 - b
        return (
            zh + a * (1 - 2 * zh),
            zl + m * (1 - 2 * zl),
            y + e * (1 - 2 * y),
            x + d * (1 - 2 * x),
        )

    def natural(a, b, e, d):
        h, l, v, u = bits(a, b, e, d)
        return pl.multiple_of((8 * h + 4 * l + 2 * v + u) * depth, depth)

    def grouped_at(a, b, e, d):
        h, l, v, u = bits(a, b, e, d)
        return pl.multiple_of((8 * h + 4 * v + 2 * l + u) * depth, depth)

    def pin_at(*k):
        return PIN.at[pl.ds(natural(*k), depth), :]

    def pout_at(*k):
        return POUT.at[:, pl.ds(natural(*k), depth)]

    def gu_at(*k):
        return GU.at[pl.ds(grouped_at(*k), depth), :]

    def dn_at(*k):
        return DN.at[pl.ds(0, hid), pl.ds(natural(*k), depth)]

    flips = {"zh": (1, 0, 0, 0), "zl": (0, 1, 0, 0), "y": (0, 0, 1, 0), "x": (0, 0, 0, 1)}

    def forward(place, sems, k, names, src=None):
        for name in names:
            there = tuple(1 - p if q else p for p, q in zip(k, flips[name]))
            push(place(*k) if src is None else src, place(*k), sems.at[rel(*there)], name)

    def start_if(condition, copy):
        @pl.when(condition)
        def _():
            copy.start()

    def arrive(place, sems, k):
        name = place.__name__ + "".join(str(bit) if isinstance(bit, int) else "v" for bit in k)
        got(place(*k), sems.at[rel(*k)], name)

    DN[pl.ds(hid, pad - hid), :] = jnp.zeros((pad - hid, width), DN.dtype)

    raw = [
        pltpu.make_async_copy(gate, RAW.at[0], local_sems.at[4]),
        pltpu.make_async_copy(up, RAW.at[1], local_sems.at[5]),
    ]
    for copy in raw:
        copy.start()
    ready = [
        pltpu.make_async_copy(source, target, local_sems.at[6 + n])
        for n, (source, target) in enumerate(
            (
                (tok_in, tok),
                (mixer_gain_in, mixer_gain),
                (gw_in, gw),
                (cs_in, cs),
                (ffn_gain_in, ffn_gain),
                (final_gain_in, final_gain),
            )
        )
    ]

    barrier = pltpu.get_barrier_semaphore()
    peers = (("c",), ("x",), ("y",), ("zl",), ("zh",), ("zl", "x"))
    for names in peers:
        pl.semaphore_signal(barrier, inc=1, device_id=other(*names), device_id_type=MESH)
    with jax.named_scope("barrier"):
        pl.semaphore_wait(barrier, len(peers))

    mine = (0, 0, 0, 0)
    quarter = 2 * fold + x
    push(tok_in, TOKR, r_misc.at[0], "c")
    forward(pin_at, r_pin, mine, ("zh", "zl", "x", "y"), pin)
    forward(pout_at, r_pout, mine, ("zh", "zl", "y", "x"), pout)
    locals_ = [
        pltpu.make_async_copy(pin, pin_at(*mine), local_sems.at[0]),
        pltpu.make_async_copy(pout, pout_at(*mine), local_sems.at[1]),
        pltpu.make_async_copy(dn.at[quarter], dn_at(*mine), local_sems.at[3]),
    ]
    for copy in locals_ + ready:
        copy.start()

    for copy in raw:
        copy.wait()
    lanes = GROUP_DIM
    low_lane = lax.broadcasted_iota(jnp.int32, (16, lanes), 1) < lanes // 2
    full = hid // lanes

    @pl.loop(0, depth // 16)
    def _(i):
        at_rows = pl.ds(pl.multiple_of(i * 16, 16), 16)
        own_rows = pl.ds(pl.multiple_of(grouped_at(*mine) + i * 16, 16), 16)

        def block(which, m):
            return RAW[which, at_rows, m * lanes : (m + 1) * lanes].astype(jnp.float32)

        def turned(which, m):
            return pltpu.roll(block(which, m), lanes // 2, 1)

        for q in range(4):
            first, skew = divmod(q * hid, lanes)
            for which in range(2):
                for j in range(full):
                    m = first + j
                    if skew == 0:
                        value = block(which, m)
                    else:
                        value = jnp.where(low_lane, turned(which, m), turned(which, m + 1))
                    start = (2 * j + which) * lanes
                    gu[q, at_rows, start : start + lanes] = value.astype(gu.dtype)
            m = first + full
            if skew == 0:
                value = jnp.where(low_lane, block(0, m), turned(1, m))
            else:
                value = jnp.where(low_lane, turned(0, m), block(1, m))
            gu[q, at_rows, 2 * full * lanes :] = value.astype(gu.dtype)
        GU[own_rows, :] = gu[quarter, at_rows, :]

    own_over = prepare(gu.at[quarter], gu_at(*mine), r_gu.at[rel(a=1)], "zh")
    start_if(fold == 1, own_over)

    trades = (((0, 0, 0, 1), ("x",)), ((0, 1, 0, 0), ("zl",)), ((0, 1, 0, 1), ("zl", "x")))

    def trade(place, sems, source, which):
        k, names = which
        _, b, _, d = k
        there = 2 * (1 - fold if b else fold) + (1 - x if d else x)
        push(source.at[there], place(*mine), sems.at[rel(*k)], *names)

    def low(l, a=0):
        return zl if l == a else 1 - zl

    def side(u):
        return x if u == 0 else 1 - x

    chunk = 32

    def normalize():
        got(TOKR, r_misc.at[0], "tok")
        for copy in ready:
            copy.wait()

        @pl.loop(0, rows // chunk)
        def _(i):
            at_rows = pl.ds(pl.multiple_of(i * chunk, chunk), chunk)
            a = tok[at_rows, :].astype(jnp.float32)
            b = TOKR[at_rows, :].astype(jnp.float32)
            mean = (
                jnp.sum(a * a, axis=1, keepdims=True) + jnp.sum(b * b, axis=1, keepdims=True)
            ) / width
            scale = lax.rsqrt(mean + EPS)
            FN[0, at_rows, :] = (a * scale * mixer_gain[c]).astype(FN.dtype)
            FN[1, at_rows, :] = (b * scale * mixer_gain[1 - c]).astype(FN.dtype)

    def across(a, b):
        arrive(pin_at, r_pin, (a, b, 0, 1))
        forward(pin_at, r_pin, (a, b, 0, 1), ("y",))
        arrive(pout_at, r_pout, (a, b, 1, 0))
        forward(pout_at, r_pout, (a, b, 1, 0), ("x",))

    across(0, 0)
    arrive(pin_at, r_pin, (1, 0, 0, 0))
    forward(pin_at, r_pin, (1, 0, 0, 0), ("zl", "x", "y"))
    arrive(pout_at, r_pout, (1, 0, 0, 0))
    forward(pout_at, r_pout, (1, 0, 0, 0), ("zl", "y", "x"))
    for k in ((0, 1, 0, 0), (1, 1, 0, 0)):
        arrive(pin_at, r_pin, k)
        forward(pin_at, r_pin, k, ("x", "y"))
        arrive(pout_at, r_pout, k)
        forward(pout_at, r_pout, k, ("y", "x"))
    trade(gu_at, r_gu, gu, trades[1])
    start_if(fold == 0, own_over)
    normalize()
    for a, b in ((1, 0), (0, 1), (1, 1)):
        across(a, b)
    forward(gu_at, r_gu, mine, ("y",), gu.at[quarter])

    def pool_part(v, n):
        total = None
        for e in range(2):
            which = c + e * (1 - 2 * c)
            for l in range(2):
                columns = pl.multiple_of((4 * l + 2 * v) * depth, 2 * depth)
                at_pin = pl.multiple_of(which * half + columns, 2 * depth)
                term = dot(
                    FN[e, :, pl.ds(columns, 2 * depth)],
                    PIN[pl.ds(at_pin, 2 * depth), n * tile : (n + 1) * tile],
                )
                total = term if total is None else total + term
        return total

    locals_[0].wait()
    for n in range(chans // tile):
        OWN[0, n] = pool_part(y, n)

    arrive(gu_at, r_gu, trades[1][0])
    forward(gu_at, r_gu, trades[1][0], ("zh", "y"))

    for a, b in ((0, 0), (1, 0), (0, 1), (1, 1)):
        for d in range(2):
            arrive(pin_at, r_pin, (a, b, 1, d))
    trade(gu_at, r_gu, gu, trades[0])
    trade(gu_at, r_gu, gu, trades[2])
    trade(dn_at, r_dn, dn, trades[1])

    groups = gw.shape[0]
    per_tile = tile // GROUP_DIM

    later = lax.broadcasted_iota(jnp.int32, (LENGTH, LENGTH), 0)
    earlier = lax.broadcasted_iota(jnp.int32, (LENGTH, LENGTH), 1)
    place_in = lax.broadcasted_iota(jnp.int32, (LENGTH, GROUP_DIM), 0)
    for n in range(chans // tile):
        pooled_in = (OWN[0, n] + pool_part(1 - y, n)).astype(jnp.bfloat16)
        for j in range(per_tile):
            g = n * per_tile + j
            window = 2 << (g % 4)
            band = ((earlier <= later) & (earlier > later - window)).astype(jnp.float32)
            band = band.astype(jnp.bfloat16)
            divisor = jnp.minimum(place_in + 1, window).astype(jnp.float32)
            for s in range(rows // LENGTH):
                grid = pooled_in[s * LENGTH : (s + 1) * LENGTH, j * GROUP_DIM : (j + 1) * GROUP_DIM]
                average = dot(band, grid) / divisor
                pooled = (average - grid.astype(jnp.float32)).astype(jnp.bfloat16)
                mapped = dot(pooled, gw[g])
                GRP[pl.ds(s * LENGTH, LENGTH), pl.ds(g * GROUP_DIM, GROUP_DIM)] = (
                    mapped * cs[:, g * GROUP_DIM : (g + 1) * GROUP_DIM]
                ).astype(GRP.dtype)

    locals_[1].wait()
    for a, b in ((0, 0), (1, 0), (0, 1), (1, 1)):
        for e in range(2):
            arrive(pout_at, r_pout, (a, b, e, 1))

    def cols_of(which, n):
        return pl.ds(pl.multiple_of(which * half + n * tile, tile), tile)

    @pl.loop(0, half // tile)
    def _(n):
        part = dot(GRP[...], POUT[:, cols_of(1 - c, n)])
        MT[:, cols_of(0, n)] = part.astype(MT.dtype)

    pool_sent = sent[:]
    sent.clear()
    push(MT, MR, r_misc.at[1], "c")

    @pl.loop(0, half // tile)
    def _(n):
        part = dot(GRP[...], POUT[:, cols_of(c, n)])
        MID[:, cols_of(0, n)] = part.astype(MID.dtype)

    arrive(gu_at, r_gu, (1, 0, 0, 0))
    forward(gu_at, r_gu, (1, 0, 0, 0), ("y",))
    got(MR, r_misc.at[1], "mix")

    @pl.loop(0, rows // chunk)
    def _(i):
        at_rows = pl.ds(pl.multiple_of(i * chunk, chunk), chunk)
        mixed = MID[at_rows, :].astype(jnp.float32) + MR[at_rows, :].astype(jnp.float32)
        middle = (tok[at_rows, :].astype(jnp.float32) + mixed).astype(jnp.bfloat16)
        MID[at_rows, :] = middle
        wide = middle.astype(jnp.float32)
        squares = jnp.sum(wide * wide, axis=1, keepdims=True)
        SQS[0, at_rows, :] = jnp.broadcast_to(squares, (chunk, SQS.shape[2]))

    push(SQS.at[0], SQR.at[0], r_misc.at[2], "c")
    got(SQR.at[0], r_misc.at[2], "sq0")

    @pl.loop(0, rows // chunk)
    def _(i):
        at_rows = pl.ds(pl.multiple_of(i * chunk, chunk), chunk)
        squares = SQS[0, at_rows, 0:1] + SQR[0, at_rows, 0:1]
        scale = lax.rsqrt(squares / width + EPS)
        wide = MID[at_rows, :].astype(jnp.float32)
        normed = (wide * scale * ffn_gain[c]).astype(SN.dtype)
        for l in range(2):
            for v in range(2):
                source = (4 * l + 2 * v) * depth
                target = (4 * v + 2 * l) * depth
                SN[0, 0, at_rows, pl.ds(target, 2 * depth)] = normed[:, source : source + 2 * depth]

    push(SN.at[0, 0], SN.at[2, 0], r_sn.at[2], "zl")
    push(SN.at[0, 0], SN.at[1, 0], r_sn.at[1], "x")
    push(SN.at[0, 0], SN.at[0, 1], r_snc.at[0], "c")

    trade(dn_at, r_dn, dn, trades[0])
    trade(dn_at, r_dn, dn, trades[2])
    for i in (0, 2):
        arrive(gu_at, r_gu, trades[i][0])
        forward(gu_at, r_gu, trades[i][0], ("zh", "y"))
    arrive(gu_at, r_gu, (1, 1, 0, 0))
    forward(gu_at, r_gu, (1, 1, 0, 0), ("y",))
    forward(dn_at, r_dn, mine, ("zh",), dn.at[quarter])
    with jax.named_scope("retire"):
        retire(pool_sent)
    got(SN.at[1, 0], r_sn.at[1], "sn1")
    push(SN.at[1, 0], SN.at[1, 1], r_snc.at[1], "c")
    arrive(dn_at, r_dn, trades[1][0])
    forward(dn_at, r_dn, trades[1][0], ("zh",))
    got(SN.at[2, 0], r_sn.at[2], "sn2")
    push(SN.at[2, 0], SN.at[3, 0], r_sn.at[3], "x")
    push(SN.at[2, 0], SN.at[2, 1], r_snc.at[2], "c")
    locals_[2].wait()
    for which in (trades[0], trades[2]):
        arrive(dn_at, r_dn, which[0])
    for l in range(2):
        forward(dn_at, r_dn, (0, low(l), 0, 1), ("zh",))

    whole_tiles = GU.shape[1] // tile
    half_tile = tile // 2
    lane = lax.broadcasted_iota(jnp.int32, (rows, half_tile), 1)
    near = jnp.where(zh == c, 0, 1)
    near_rows = pl.ds(pl.multiple_of(zh * half, half), half)
    quart = half // 2

    def far_part(v):
        rows_at = pl.multiple_of((1 - zh) * half + v * quart, quart)
        return pl.ds(rows_at, quart), pl.ds(pl.multiple_of(v * quart, quart), quart)

    own_rows_far, own_cols_far = far_part(y)
    end_rows_far, end_cols_far = far_part(1 - y)
    last = pl.ds(whole_tiles * tile, half_tile)

    def tile_at(j, size):
        return pl.ds(pl.multiple_of(j * size, size), size)

    def begin(r):
        got(SN.at[r, 1], r_snc.at[r], f"snc{r}")
        with jax.named_scope(f"begin{r}"):

            @pl.loop(0, whole_tiles)
            def _(j):
                ACC[r, :, tile_at(j, tile)] = dot(SN[r, near], GU[near_rows, tile_at(j, tile)])

            ACC[r, :, last] = dot(SN[r, near], GU[near_rows, last])

    def more(r):
        with jax.named_scope(f"more{r}"):
            left = SN.at[r, 1 - near, :, own_cols_far]

            @pl.loop(0, whole_tiles)
            def _(j):
                here = tile_at(j, tile)
                ACC[r, :, here] = ACC[r, :, here] + dot(left[...], GU[own_rows_far, here])

            ACC[r, :, last] = ACC[r, :, last] + dot(left[...], GU[own_rows_far, last])

    def gated(r):
        left = SN.at[r, 1 - near, :, end_cols_far]
        with jax.named_scope(f"gated{r}"):

            @pl.loop(0, whole_tiles)
            def _(j):
                both = dot(left[...], GU[end_rows_far, tile_at(j, tile)])
                both = both + ACC[r, :, tile_at(j, tile)]
                gate, up = both[:, :half_tile], both[:, half_tile:]
                value = gate / (1.0 + jnp.exp(-gate)) * up
                H[r, :, tile_at(j, half_tile)] = value.astype(H.dtype)

            both = dot(left[...], GU[end_rows_far, last]) + ACC[r, :, last]
            up = pltpu.roll(both, half_tile // 2, 1)
            value = both / (1.0 + jnp.exp(-both)) * up
            H[r, :, pl.ds(whole_tiles * half_tile, half_tile)] = jnp.where(
                lane < half_tile // 2, value, 0.0
            ).astype(H.dtype)

    for b, d in ((0, 0), (0, 1), (1, 0), (1, 1)):
        arrive(gu_at, r_gu, (0, b, 1, d))
    begin(0)
    arrive(gu_at, r_gu, (1, 0, 0, 1))
    forward(gu_at, r_gu, (1, 0, 0, 1), ("y",))
    begin(1)
    begin(2)
    arrive(gu_at, r_gu, (1, 1, 0, 1))
    forward(gu_at, r_gu, (1, 1, 0, 1), ("y",))
    more(0)
    more(1)
    got(SN.at[3, 0], r_sn.at[3], "sn3")
    push(SN.at[3, 0], SN.at[3, 1], r_snc.at[3], "c")
    for l in range(2):
        for u in range(2):
            forward(dn_at, r_dn, (0, low(l), 0, side(u)), ("y",))
    more(2)
    begin(3)
    more(3)
    for b, d in ((0, 0), (0, 1), (1, 0), (1, 1)):
        arrive(gu_at, r_gu, (1, b, 1, d))
    whole_steps = [(a, e, l, None) for a in range(2) for e in range(2) for l in range(2)]
    steps = whole_steps[:-1] + [whole_steps[-1][:3] + (u,) for u in range(2)]
    firsts = ("x", "zl")
    owners = (zh == c, zh != c)
    role_sent = ([], [])

    def role_copy(which, *args):
        src, dst, rsem, *names = args
        copy = remote(src, dst, SENDS + len(role_sent[which]), rsem, *names)
        role_sent[which].append(copy)
        return copy

    def place_of(s):
        a, _, _, u = steps[s]
        slot = min(s - 4 * a, 3)
        start, size = (0, tile) if u is None else (u * half_tile, half_tile)
        return a, slot, s - 4 * a, pl.ds(start, size)

    def step_cols(s, which=0):
        _, e, l, u = steps[s]
        v = y + e * (1 - 2 * y)
        start, size = (0, tile) if u is None else (u * half_tile, half_tile)
        return pl.ds(pl.multiple_of(which * half + (2 * l + v) * tile + start, size), size)

    def produce(s, blocks=(0, 1, 2, 3)):
        a, t, i, part = place_of(s)
        columns = step_cols(s, zh + a * (1 - 2 * zh))
        single = s >= 2
        if single:
            ways = [(TS.at[t, :, :, part], TR.at[t, :, :, part], r_tp.at[tp_index(s)])]
        else:
            ways = [(TS.at[t, r], TR.at[t, r], r_tp.at[tp_index(s) + r]) for r in blocks]
        overs = [role_copy(1 - a, *way, "c") for way in ways]

        @pl.when(owners[1 - a])
        def _():
            for n, r in enumerate(blocks):
                TS[t, r, :, part] = dot(H[r], DN[:, columns]).astype(TS.dtype)
                if not single:
                    overs[n].start()
            if single:
                overs[0].start()

        @pl.when(owners[a])
        def _():
            for r in blocks:
                OWN[t, r, :, part] = dot(H[r], DN[:, columns])

    def tp_index(s):
        a, t, i, part = place_of(s)
        return i if a else (4 * s if s < 2 else 6 + s)

    def crossed(s):
        a, t, i, part = place_of(s)
        got(TR.at[t, :, :, part], r_tp.at[tp_index(s)], f"tp{s}")

    def both_cores(s, r):
        a, t, i, part = place_of(s)
        if s < 2:
            got(TR.at[t, r], r_tp.at[tp_index(s) + r], f"tp{s}r{r}")
        return OWN[t, r, :, part] + TR[t, r, :, part].astype(jnp.float32)

    def halves_of(axis):
        return ((1, 3), (0, 2)) if axis == "x" else ((2, 3), (0, 1))

    def first_stage(s):
        a, t, i, part = place_of(s)
        axis = firsts[s % 2]
        over = role_copy(a, S1.at[t], R1.at[t], r_s1.at[i], axis)

        @pl.when(owners[a])
        def _():
            if s >= 2:
                crossed(s)
            for n, r in enumerate(halves_of(axis)[0]):
                S1[t, n] = both_cores(s, r).astype(S1.dtype)
            over.start()

    def second_stage(s):
        a, t, i, part = place_of(s)
        over = role_copy(a, S2.at[t], R2.at[t], r_s2.at[i], firsts[1 - s % 2])
        keep, give = halves_of(firsts[s % 2])[1]

        @pl.when(owners[a])
        def _():
            given = both_cores(s, give)
            got(R1.at[t], r_s1.at[i], f"first{s}")
            S2[t] = (given + R1[t, 1].astype(jnp.float32)).astype(S2.dtype)
            over.start()
            CL[t] = both_cores(s, keep) + R1[t, 0].astype(jnp.float32)

    def close(s, t, part, columns, summed):
        closing = MID[:, columns].astype(jnp.float32) + summed
        CL[t, :, part] = closing
        squares = jnp.sum(closing * closing, axis=1, keepdims=True)
        squares = jnp.broadcast_to(squares, SQS.shape[1:])
        SQS[1] = squares if t == 0 else SQS[1] + squares

    def finish(s):
        a, t, i, part = place_of(s)
        columns = step_cols(s)

        @pl.when(owners[a])
        def _():
            got(R2.at[t], r_s2.at[i], f"second{s}")
            close(s, t, part, columns, CL[t] + R2[t].astype(jnp.float32))

    def straight(t, part):
        return (
            (3, S2.at[t, :, part], R2.at[t, :, part], r_s2, ("zl", "x")),
            (1, S1.at[t, 0, :, part], R1.at[t, 0, :, part], r_s1, ("x",)),
            (2, S1.at[t, 1, :, part], R1.at[t, 1, :, part], r_s3, ("zl",)),
        )

    def scatter(s):
        a, t, i, part = place_of(s)
        ways = straight(t, part)
        overs = [
            role_copy(a, source, target, sems.at[i], *names)
            for _, source, target, sems, names in ways
        ]

        @pl.when(owners[a])
        def _():
            crossed(s)
            for (r, source, _, _, _), over in zip(ways, overs):
                source[...] = both_cores(s, r).astype(S1.dtype)
                over.start()
            CL[t, :, part] = both_cores(s, 0)

    def gather_sums(s):
        a, t, i, part = place_of(s)
        columns = step_cols(s)

        @pl.when(owners[a])
        def _():
            summed = CL[t, :, part]
            for r, _, target, sems, _ in straight(t, part):
                got(target, sems.at[i], f"sum{s}from{r}")
                summed = summed + target[...].astype(jnp.float32)
            close(s, t, part, columns, summed)

    def relay(l):
        for d in range(2):
            k = (1, low(l, 1), 0, d)
            arrive(dn_at, r_dn, k)
            forward(dn_at, r_dn, k, ("y",))

    def landed(a, l, which=(0, 1)):
        for u in which:
            arrive(dn_at, r_dn, (a, low(l, a), 1, side(u)))

    gated(3)
    gated(1)
    produce(0, (1, 3))
    gated(2)
    produce(1, (2, 3))
    first_stage(0)
    gated(0)
    produce(0, (0, 2))
    produce(1, (0, 1))
    first_stage(1)
    landed(0, 0)
    produce(2)
    relay(0)
    produce(4)
    first_stage(2)
    landed(0, 1)
    produce(3)
    first_stage(4)
    second_stage(0)
    second_stage(1)
    first_stage(3)
    relay(1)
    produce(5)
    first_stage(5)
    landed(1, 0)
    produce(6)
    first_stage(6)
    landed(1, 1, (0,))
    produce(7)
    for s in (2, 3, 4):
        second_stage(s)
    scatter(7)
    second_stage(5)
    landed(1, 1, (1,))
    produce(8)
    scatter(8)
    second_stage(6)
    for s in range(7):
        finish(s)
    for s in (7, 8):
        gather_sums(s)
    push(SQS.at[1], SQR.at[1], r_misc.at[3], "c")
    got(SQR.at[1], r_misc.at[3], "sq1")
    scale = lax.rsqrt((SQS[1, :, 0:1] + SQR[1, :, 0:1]) / width + EPS)
    finals = []
    for t in range(4):
        columns = step_cols(t)
        OUT[:, columns] = (CL[t] * scale * final_gain[:, columns]).astype(out.dtype)
        copy = pltpu.make_async_copy(
            OUT.at[:, columns], out.at[:, columns], local_sems.at[12 + t]
        )
        copy.start()
        finals.append(copy)

    with jax.named_scope("drain"):
        retire(sent)
        for which in range(2):

            @pl.when(owners[which])
            def _():
                for copy in role_sent[which]:
                    copy.wait_send()

        for copy in finals:
            copy.wait()


def fused(
    tokens,
    mixer_gain,
    pool_input,
    group_weight,
    channel_scale,
    pool_output,
    ffn_gain,
    gate_weight,
    up_weight,
    down_weight,
    final_gain,
):
    rows, half = tokens.shape
    depth, hidden_all = gate_weight.shape
    hid = hidden_all // 4
    full = hid // GROUP_DIM
    chans = pool_input.shape[1]
    dn = down_weight.reshape(4, hid, depth)
    pad = (full + 1) * GROUP_DIM
    bf, f32 = jnp.bfloat16, jnp.float32
    hbm = pl.BlockSpec(memory_space=pl.ANY)
    dma = pltpu.SemaphoreType.DMA
    tile = 256
    scratch = [
        pltpu.VMEM((rows, half), bf),
        pltpu.VMEM((1, half), f32),
        pltpu.VMEM((rows, half), bf),
        pltpu.VMEM((2, 1, half), f32),
        pltpu.VMEM(group_weight.shape, bf),
        pltpu.VMEM((1, chans), f32),
        pltpu.VMEM((2, 1, half), f32),
        pltpu.VMEM((2, depth, hidden_all), bf),
        pltpu.VMEM((4, depth, 2 * hid), bf),
        pltpu.VMEM((rows, half), bf),
        pltpu.VMEM((2, rows, half), bf),
        pltpu.VMEM((2 * half, chans), bf),
        pltpu.VMEM((chans, 2 * half), bf),
        pltpu.VMEM((rows, chans), bf),
        pltpu.VMEM((rows, half), bf),
        pltpu.VMEM((rows, half), bf),
        pltpu.VMEM((rows, half), bf),
        pltpu.VMEM((2, rows, GROUP_DIM), f32),
        pltpu.VMEM((2, rows, GROUP_DIM), f32),
        pltpu.VMEM((4, 2, rows, half), bf),
        pltpu.VMEM((2 * half, 2 * hid), bf),
        pltpu.VMEM((pad, 2 * half), bf),
        pltpu.VMEM((4, rows, 2 * hid), f32),
        pltpu.VMEM((4, rows, pad), bf),
        pltpu.VMEM((4, 4, rows, tile), bf),
        pltpu.VMEM((4, 4, rows, tile), bf),
        pltpu.VMEM((4, 4, rows, tile), f32),
        pltpu.VMEM((4, 2, rows, tile), bf),
        pltpu.VMEM((4, 2, rows, tile), bf),
        pltpu.VMEM((4, rows, tile), bf),
        pltpu.VMEM((4, rows, tile), bf),
        pltpu.VMEM((4, rows, tile), f32),
        dma((SENDS + ROLE_SENDS,)),
        dma((16,)),
        dma((PIECES,)),
        dma((PIECES,)),
        dma((PIECES,)),
        dma((PIECES,)),
        dma((4,)),
        dma((4,)),
        dma((4,)),
        dma((10,)),
        dma((5,)),
        dma((5,)),
        dma((5,)),
    ]
    return pl.pallas_call(
        kernel,
        out_shape=jax.ShapeDtypeStruct((rows, half), bf),
        in_specs=[hbm] * 11,
        out_specs=hbm,
        scratch_shapes=scratch,
        compiler_params=pltpu.CompilerParams(
            collective_id=0, has_side_effects=True, vmem_limit_bytes=67043328
        ),
    )(
        tokens,
        mixer_gain.reshape(2, 1, half),
        pool_input,
        group_weight,
        channel_scale.reshape(1, chans),
        pool_output,
        ffn_gain.reshape(2, 1, half),
        gate_weight,
        up_weight,
        dn,
        final_gain.reshape(1, half),
    )


def solution(mesh):
    fs, tp = mesh.shape["fs"], mesh.shape["tp"]
    if fs != PIECES or tp != 2:
        return general(mesh)
    split = Mesh(mesh.devices.reshape(2, 2, 2, 2, 2), AXES)
    rows = AXES[:4]
    placed = (
        P(rows, "c"),
        P(),
        P(rows, "c"),
        P("c", None, None),
        P("c"),
        P("c", rows),
        P(),
        P(rows, "c"),
        P(rows, "c"),
        P("c", rows),
        P("c"),
    )
    return jax.shard_map(
        fused, mesh=split, in_specs=placed, out_specs=P(rows, "c"), check_vma=False
    )
```

```python
import functools

import jax
import jax.numpy as jnp
from jax import lax
from jax.experimental import pallas as pl
from jax.experimental.pallas import tpu as pltpu
from jax.sharding import Mesh, PartitionSpec as P

GROUP_DIM = 128
LENGTH = 128
EPS = 1e-06
INNER = 4


def partner(at, step, count):
    if count & (count - 1) == 0:
        return at ^ step, at ^ step
    return (at + step) % count, (at - step) % count


def send(value, axis, count, step):
    pairs = [(at, partner(at, step, count)[0]) for at in range(count)]
    return lax.ppermute(value, axis, pairs)


def place(whole, piece, at, dim):
    return lax.dynamic_update_slice_in_dim(whole, piece, at * piece.shape[dim], dim)


def gather(value, axis, dim):
    count = lax.axis_size(axis)
    me = lax.axis_index(axis)
    shape = list(value.shape)
    shape[dim] *= count
    pieces = [(me, value)]
    for step in range(1, count):
        pieces.append((partner(me, step, count)[1], send(value, axis, count, step)))
    whole = jnp.zeros(shape, value.dtype)
    for at, piece in pieces:
        whole = place(whole, piece, at, dim)
    return whole


def exchange(value, axis, cut, dim):
    count = lax.axis_size(axis)
    me = lax.axis_index(axis)
    width = value.shape[cut] // count
    block = lambda at: lax.dynamic_slice_in_dim(value, at * width, width, cut)
    pieces = [(me, block(me))]
    for step in range(1, count):
        there, origin = partner(me, step, count)
        pieces.append((origin, send(block(there), axis, count, step)))
    shape = list(pieces[0][1].shape)
    shape[dim] *= count
    whole = jnp.zeros(shape, value.dtype)
    for at, piece in pieces:
        whole = place(whole, piece, at, dim)
    return whole


def scatter_sum(value, axis, dim):
    count = lax.axis_size(axis)
    me = lax.axis_index(axis)
    width = value.shape[dim] // count
    block = lambda at: lax.dynamic_slice_in_dim(value, at * width, width, dim)
    total = block(me).astype(jnp.float32)
    for step in range(1, count):
        there = partner(me, step, count)[0]
        total = total + send(block(there), axis, count, step).astype(jnp.float32)
    return total


def ring(value, axis, dim, first=None, behind=None):
    count = lax.axis_size(axis)
    me = lax.axis_index(axis)
    shape = list(value.shape)
    shape[dim] *= count
    whole = place(jnp.zeros(shape, value.dtype), value, me, dim)
    ahead = [(at, (at + 1) % count) for at in range(count)]
    back = [(at, (at - 1) % count) for at in range(count)]
    up = down = value
    for step in range(1, count // 2 + 1):
        if step == 1 and first is not None:
            up = first
        else:
            up = lax.ppermute(up, axis, ahead)
        whole = place(whole, up, (me - step) % count, dim)
        if 2 * step < count:
            if step == 1 and behind is not None:
                down = behind
            else:
                down = lax.ppermute(down, axis, back)
            whole = place(whole, down, (me + step) % count, dim)
    return whole


def half_norm(values, gain, width):
    wide = values.astype(jnp.float32)
    squares = lax.psum(jnp.sum(wide * wide, axis=1, keepdims=True), "tp")
    return wide * lax.rsqrt(squares / width + EPS) * gain


def dot(left, right):
    return jnp.dot(left, right, preferred_element_type=jnp.float32)


def local(
    tokens,
    mixer_gain,
    pool_input,
    group_weight,
    channel_scale,
    pool_output,
    ffn_gain,
    gate_weight,
    up_weight,
    down_weight,
    final_gain,
):
    tp = lax.axis_index("tp")
    columns = tokens.shape[1]
    width = columns * lax.axis_size("tp")
    inner = lax.axis_size("inner")

    full_rows = gather(tokens, "tp", 1)
    depth, hidden_all = gate_weight.shape
    hidden_width = hidden_all // inner
    both = jnp.concatenate(
        [
            gate_weight.reshape(depth, inner, hidden_width),
            up_weight.reshape(depth, inner, hidden_width),
        ],
        axis=2,
    ).reshape(depth, inner * 2 * hidden_width)
    pool_in = ring(pool_input[None, None], "outer", 0)
    pool_out = ring(pool_output[None, None], "outer", 0)
    both = exchange(both, "inner", 1, 0)
    pool_in, pool_out, both = lax.optimization_barrier((pool_in, pool_out, both))
    pool_in = gather(pool_in, "inner", 1).reshape(width, pool_input.shape[1])
    down_weight, pool_in = lax.optimization_barrier((down_weight, pool_in))
    pool_out = gather(pool_out, "inner", 1)
    pool_out = jnp.transpose(pool_out, (2, 0, 1, 3)).reshape(pool_output.shape[0], width)
    planes = lax.axis_size("outer")
    first = lax.ppermute(both, "outer", [(at, (at + 1) % planes) for at in range(planes)])
    behind = lax.ppermute(both, "outer", [(at, (at - 1) % planes) for at in range(planes)])
    down = exchange(down_weight, "inner", 0, 1)

    wide = full_rows.astype(jnp.float32)
    first_normed = (
        wide * lax.rsqrt(jnp.mean(wide * wide, axis=-1, keepdims=True) + EPS) * mixer_gain
    ).astype(jnp.bfloat16)
    row_count = first_normed.shape[0]
    pooled_in = dot(first_normed, pool_in).astype(jnp.bfloat16)
    local_groups = group_weight.shape[0]
    group_ids = tp * local_groups + jnp.arange(local_groups, dtype=jnp.int32)
    windows = jnp.left_shift(jnp.int32(2), group_ids % 4)
    later = jnp.arange(LENGTH, dtype=jnp.int32)[None, :, None]
    earlier = jnp.arange(LENGTH, dtype=jnp.int32)[None, None, :]
    reach = windows[:, None, None]
    inside = (earlier <= later) & (earlier > later - reach)
    band = inside.astype(jnp.bfloat16)
    divisor = jnp.minimum(later[:, :, 0] + 1, windows[:, None]).astype(jnp.float32)
    grid_low = pooled_in.reshape(row_count // LENGTH, LENGTH, local_groups, GROUP_DIM)
    window_sums = jnp.einsum("gts,nsgc->ntgc", band, grid_low, preferred_element_type=jnp.float32)
    average = window_sums / jnp.transpose(divisor)[None, :, :, None]
    pooled = (
        (average - grid_low.astype(jnp.float32))
        .astype(jnp.bfloat16)
        .reshape(row_count, local_groups, GROUP_DIM)
    )
    mapped = jnp.einsum("ngc,gcd->ngd", pooled, group_weight, preferred_element_type=jnp.float32)
    grouped = (mapped.reshape(row_count, local_groups * GROUP_DIM) * channel_scale).astype(
        jnp.bfloat16
    )
    mixer_terms = dot(grouped, pool_out).astype(jnp.bfloat16)
    mixer_terms, first, behind, both, down = lax.optimization_barrier(
        (mixer_terms, first, behind, both, down)
    )
    both = ring(both, "outer", 0, first, behind)
    mixer_out = scatter_sum(mixer_terms, "tp", 1)
    middle = (tokens.astype(jnp.float32) + mixer_out).astype(jnp.bfloat16)

    own_gain = lax.dynamic_slice_in_dim(ffn_gain, tp * columns, columns, 0)
    second_half = half_norm(middle, own_gain, width).astype(jnp.bfloat16)
    ahead = lax.ppermute(down, "outer", [(at, (at + 1) % planes) for at in range(planes)])
    after = lax.ppermute(down, "outer", [(at, (at - 1) % planes) for at in range(planes)])
    second_half, both, ahead, after, down = lax.optimization_barrier(
        (gather(second_half, "inner", 0), both, ahead, after, down)
    )
    down = ring(down, "outer", 1, ahead, after)
    second_normed = gather(second_half, "tp", 1)
    gate = dot(second_normed, both[:, :hidden_width])
    upward = dot(second_normed, both[:, hidden_width:])
    hidden = (jax.nn.silu(gate) * upward).astype(jnp.bfloat16)
    ffn_terms = dot(hidden, down).astype(jnp.bfloat16)
    over_cores = scatter_sum(ffn_terms, "tp", 1).astype(jnp.bfloat16)
    ffn_out = scatter_sum(over_cores, "inner", 0)
    closing = middle.astype(jnp.float32) + ffn_out
    return half_norm(closing, final_gain, width).astype(jnp.bfloat16)


def general(mesh):
    fs, tp = mesh.shape["fs"], mesh.shape["tp"]
    inner = INNER if fs % INNER == 0 else 1
    split = Mesh(mesh.devices.reshape(fs // inner, inner, tp), ("outer", "inner", "tp"))
    rows = ("outer", "inner")
    placed = (
        P(rows, "tp"),
        P(),
        P(rows, "tp"),
        P("tp", None, None),
        P("tp"),
        P("tp", rows),
        P(),
        P(rows, "tp"),
        P(rows, "tp"),
        P("tp", rows),
        P("tp"),
    )
    return jax.shard_map(
        local, mesh=split, in_specs=placed, out_specs=P(rows, "tp"), check_vma=False
    )


AXES = ("zh", "zl", "y", "x", "c")
MESH = pl.DeviceIdType.MESH
PIECES = 16
SENDS = 56
ROLE_SENDS = 22


def rel(a=0, b=0, e=0, d=0):
    return 8 * a + 4 * b + 2 * e + d


def kernel(
    tok_in,
    mixer_gain_in,
    pin,
    gw_in,
    cs_in,
    pout,
    ffn_gain_in,
    gate,
    up,
    dn,
    final_gain_in,
    out,
    OUT,
    final_gain,
    tok,
    mixer_gain,
    gw,
    cs,
    ffn_gain,
    RAW,
    gu,
    TOKR,
    FN,
    PIN,
    POUT,
    GRP,
    MT,
    MR,
    MID,
    SQS,
    SQR,
    SN,
    GU,
    DN,
    ACC,
    H,
    TS,
    TR,
    OWN,
    S1,
    R1,
    S2,
    R2,
    CL,
    send_sems,
    local_sems,
    r_pin,
    r_pout,
    r_gu,
    r_dn,
    r_misc,
    r_sn,
    r_snc,
    r_tp,
    r_s1,
    r_s2,
    r_s3,
):
    at = {name: lax.axis_index(name) for name in AXES}
    zh, zl, y, x, c = (at[name] for name in AXES)
    rows, half = tok.shape
    depth = pin.shape[0]
    hid = dn.shape[1]
    pad = H.shape[2]
    chans = pin.shape[1]
    width = 2 * half
    tile = 256

    fold = zl + zh - 2 * zl * zh

    def other(*names):
        flip = {n: n in names for n in AXES}
        flip["zl"] = flip["zl"] != flip["zh"]
        return tuple(1 - at[n] if flip[n] else at[n] for n in AXES)

    sent = []
    spare = list(range(SENDS))

    def remote(src, dst, ssem, rsem, *names):
        return pltpu.make_async_remote_copy(
            src_ref=src,
            dst_ref=dst,
            send_sem=send_sems.at[ssem],
            recv_sem=rsem,
            device_id=other(*names),
            device_id_type=MESH,
        )

    def prepare(src, dst, rsem, *names):
        ssem = spare.pop(0)
        copy = remote(src, dst, ssem, rsem, *names)
        sent.append((copy, ssem))
        return copy

    def push(src, dst, rsem, *names):
        prepare(src, dst, rsem, *names).start()

    def retire(copies):
        for copy, ssem in copies:
            copy.wait_send()
            spare.append(ssem)
        copies.clear()

    def got(dst, rsem, name):
        with jax.named_scope("wait_" + name):
            pltpu.make_async_remote_copy(
                src_ref=dst,
                dst_ref=dst,
                send_sem=send_sems.at[0],
                recv_sem=rsem,
                device_id=other("c"),
                device_id_type=MESH,
            ).wait_recv()

    def bits(a, b, e, d):
        m = b if a == 0 else 1 - b
        return (
            zh + a * (1 - 2 * zh),
            zl + m * (1 - 2 * zl),
            y + e * (1 - 2 * y),
            x + d * (1 - 2 * x),
        )

    def natural(a, b, e, d):
        h, l, v, u = bits(a, b, e, d)
        return pl.multiple_of((8 * h + 4 * l + 2 * v + u) * depth, depth)

    def grouped_at(a, b, e, d):
        h, l, v, u = bits(a, b, e, d)
        return pl.multiple_of((8 * h + 4 * v + 2 * l + u) * depth, depth)

    def pin_at(*k):
        return PIN.at[pl.ds(natural(*k), depth), :]

    def pout_at(*k):
        return POUT.at[:, pl.ds(natural(*k), depth)]

    def gu_at(*k):
        return GU.at[pl.ds(grouped_at(*k), depth), :]

    def dn_at(*k):
        return DN.at[pl.ds(0, hid), pl.ds(natural(*k), depth)]

    flips = {"zh": (1, 0, 0, 0), "zl": (0, 1, 0, 0), "y": (0, 0, 1, 0), "x": (0, 0, 0, 1)}

    def forward(place, sems, k, names, src=None):
        for name in names:
            there = tuple(1 - p if q else p for p, q in zip(k, flips[name]))
            push(place(*k) if src is None else src, place(*k), sems.at[rel(*there)], name)

    def start_if(condition, copy):
        @pl.when(condition)
        def _():
            copy.start()

    def arrive(place, sems, k):
        name = place.__name__ + "".join(str(bit) if isinstance(bit, int) else "v" for bit in k)
        got(place(*k), sems.at[rel(*k)], name)

    DN[pl.ds(hid, pad - hid), :] = jnp.zeros((pad - hid, width), DN.dtype)

    raw = [
        pltpu.make_async_copy(gate, RAW.at[0], local_sems.at[4]),
        pltpu.make_async_copy(up, RAW.at[1], local_sems.at[5]),
    ]
    for copy in raw:
        copy.start()
    ready = [
        pltpu.make_async_copy(source, target, local_sems.at[6 + n])
        for n, (source, target) in enumerate(
            (
                (tok_in, tok),
                (mixer_gain_in, mixer_gain),
                (gw_in, gw),
                (cs_in, cs),
                (ffn_gain_in, ffn_gain),
                (final_gain_in, final_gain),
            )
        )
    ]

    barrier = pltpu.get_barrier_semaphore()
    peers = (("c",), ("x",), ("y",), ("zl",), ("zh",), ("zl", "x"))
    for names in peers:
        pl.semaphore_signal(barrier, inc=1, device_id=other(*names), device_id_type=MESH)
    with jax.named_scope("barrier"):
        pl.semaphore_wait(barrier, len(peers))

    mine = (0, 0, 0, 0)
    quarter = 2 * fold + x
    push(tok_in, TOKR, r_misc.at[0], "c")
    forward(pin_at, r_pin, mine, ("zh", "zl", "x", "y"), pin)
    forward(pout_at, r_pout, mine, ("zh", "zl", "y", "x"), pout)
    locals_ = [
        pltpu.make_async_copy(pin, pin_at(*mine), local_sems.at[0]),
        pltpu.make_async_copy(pout, pout_at(*mine), local_sems.at[1]),
        pltpu.make_async_copy(dn.at[quarter], dn_at(*mine), local_sems.at[3]),
    ]
    for copy in locals_ + ready:
        copy.start()

    for copy in raw:
        copy.wait()
    lanes = GROUP_DIM
    low_lane = lax.broadcasted_iota(jnp.int32, (16, lanes), 1) < lanes // 2
    full = hid // lanes

    @pl.loop(0, depth // 16)
    def _(i):
        at_rows = pl.ds(pl.multiple_of(i * 16, 16), 16)
        own_rows = pl.ds(pl.multiple_of(grouped_at(*mine) + i * 16, 16), 16)

        def block(which, m):
            return RAW[which, at_rows, m * lanes : (m + 1) * lanes].astype(jnp.float32)

        def turned(which, m):
            return pltpu.roll(block(which, m), lanes // 2, 1)

        for q in range(4):
            first, skew = divmod(q * hid, lanes)
            for which in range(2):
                for j in range(full):
                    m = first + j
                    if skew == 0:
                        value = block(which, m)
                    else:
                        value = jnp.where(low_lane, turned(which, m), turned(which, m + 1))
                    start = (2 * j + which) * lanes
                    gu[q, at_rows, start : start + lanes] = value.astype(gu.dtype)
            m = first + full
            if skew == 0:
                value = jnp.where(low_lane, block(0, m), turned(1, m))
            else:
                value = jnp.where(low_lane, turned(0, m), block(1, m))
            gu[q, at_rows, 2 * full * lanes :] = value.astype(gu.dtype)
        GU[own_rows, :] = gu[quarter, at_rows, :]

    own_over = prepare(gu.at[quarter], gu_at(*mine), r_gu.at[rel(a=1)], "zh")
    start_if(fold == 1, own_over)

    trades = (((0, 0, 0, 1), ("x",)), ((0, 1, 0, 0), ("zl",)), ((0, 1, 0, 1), ("zl", "x")))

    def trade(place, sems, source, which):
        k, names = which
        _, b, _, d = k
        there = 2 * (1 - fold if b else fold) + (1 - x if d else x)
        push(source.at[there], place(*mine), sems.at[rel(*k)], *names)

    def low(l, a=0):
        return zl if l == a else 1 - zl

    def side(u):
        return x if u == 0 else 1 - x

    chunk = 64

    def normalize():
        got(TOKR, r_misc.at[0], "tok")
        for copy in ready:
            copy.wait()

        @pl.loop(0, rows // chunk)
        def _(i):
            at_rows = pl.ds(pl.multiple_of(i * chunk, chunk), chunk)
            a = tok[at_rows, :].astype(jnp.float32)
            b = TOKR[at_rows, :].astype(jnp.float32)
            mean = (
                jnp.sum(a * a, axis=1, keepdims=True) + jnp.sum(b * b, axis=1, keepdims=True)
            ) / width
            scale = lax.rsqrt(mean + EPS)
            FN[0, at_rows, :] = (a * scale * mixer_gain[c]).astype(FN.dtype)
            FN[1, at_rows, :] = (b * scale * mixer_gain[1 - c]).astype(FN.dtype)

    def across(a, b):
        arrive(pin_at, r_pin, (a, b, 0, 1))
        forward(pin_at, r_pin, (a, b, 0, 1), ("y",))
        arrive(pout_at, r_pout, (a, b, 1, 0))
        forward(pout_at, r_pout, (a, b, 1, 0), ("x",))

    across(0, 0)
    arrive(pin_at, r_pin, (1, 0, 0, 0))
    forward(pin_at, r_pin, (1, 0, 0, 0), ("zl", "x", "y"))
    arrive(pout_at, r_pout, (1, 0, 0, 0))
    forward(pout_at, r_pout, (1, 0, 0, 0), ("zl", "y", "x"))
    for k in ((0, 1, 0, 0), (1, 1, 0, 0)):
        arrive(pin_at, r_pin, k)
        forward(pin_at, r_pin, k, ("x", "y"))
        arrive(pout_at, r_pout, k)
        forward(pout_at, r_pout, k, ("y", "x"))
    trade(gu_at, r_gu, gu, trades[1])
    start_if(fold == 0, own_over)
    normalize()
    for a, b in ((1, 0), (0, 1), (1, 1)):
        across(a, b)
    forward(gu_at, r_gu, mine, ("y",), gu.at[quarter])

    def pool_part(v, n):
        total = None
        for e in range(2):
            which = c + e * (1 - 2 * c)
            for l in range(2):
                columns = pl.multiple_of((4 * l + 2 * v) * depth, 2 * depth)
                at_pin = pl.multiple_of(which * half + columns, 2 * depth)
                term = dot(
                    FN[e, :, pl.ds(columns, 2 * depth)],
                    PIN[pl.ds(at_pin, 2 * depth), n * tile : (n + 1) * tile],
                )
                total = term if total is None else total + term
        return total

    locals_[0].wait()
    for n in range(chans // tile):
        OWN[0, n] = pool_part(y, n)

    arrive(gu_at, r_gu, trades[1][0])
    forward(gu_at, r_gu, trades[1][0], ("zh", "y"))

    for a, b in ((0, 0), (1, 0), (0, 1), (1, 1)):
        for d in range(2):
            arrive(pin_at, r_pin, (a, b, 1, d))
    trade(gu_at, r_gu, gu, trades[0])
    trade(gu_at, r_gu, gu, trades[2])
    trade(dn_at, r_dn, dn, trades[1])

    groups = gw.shape[0]
    per_tile = tile // GROUP_DIM

    later = lax.broadcasted_iota(jnp.int32, (LENGTH, LENGTH), 0)
    earlier = lax.broadcasted_iota(jnp.int32, (LENGTH, LENGTH), 1)
    place_in = lax.broadcasted_iota(jnp.int32, (LENGTH, GROUP_DIM), 0)
    for n in range(chans // tile):
        pooled_in = (OWN[0, n] + pool_part(1 - y, n)).astype(jnp.bfloat16)
        for j in range(per_tile):
            g = n * per_tile + j
            window = 2 << (g % 4)
            band = ((earlier <= later) & (earlier > later - window)).astype(jnp.float32)
            band = band.astype(jnp.bfloat16)
            divisor = jnp.minimum(place_in + 1, window).astype(jnp.float32)
            for s in range(rows // LENGTH):
                grid = pooled_in[s * LENGTH : (s + 1) * LENGTH, j * GROUP_DIM : (j + 1) * GROUP_DIM]
                average = dot(band, grid) / divisor
                pooled = (average - grid.astype(jnp.float32)).astype(jnp.bfloat16)
                mapped = dot(pooled, gw[g])
                GRP[pl.ds(s * LENGTH, LENGTH), pl.ds(g * GROUP_DIM, GROUP_DIM)] = (
                    mapped * cs[:, g * GROUP_DIM : (g + 1) * GROUP_DIM]
                ).astype(GRP.dtype)

    locals_[1].wait()
    for a, b in ((0, 0), (1, 0), (0, 1), (1, 1)):
        for e in range(2):
            arrive(pout_at, r_pout, (a, b, e, 1))

    def cols_of(which, n):
        return pl.ds(pl.multiple_of(which * half + n * tile, tile), tile)

    @pl.loop(0, half // tile)
    def _(n):
        part = dot(GRP[...], POUT[:, cols_of(1 - c, n)])
        MT[:, cols_of(0, n)] = part.astype(MT.dtype)

    pool_sent = sent[:]
    sent.clear()
    push(MT, MR, r_misc.at[1], "c")

    @pl.loop(0, half // tile)
    def _(n):
        part = dot(GRP[...], POUT[:, cols_of(c, n)])
        MID[:, cols_of(0, n)] = part.astype(MID.dtype)

    arrive(gu_at, r_gu, (1, 0, 0, 0))
    forward(gu_at, r_gu, (1, 0, 0, 0), ("y",))
    got(MR, r_misc.at[1], "mix")

    @pl.loop(0, rows // chunk)
    def _(i):
        at_rows = pl.ds(pl.multiple_of(i * chunk, chunk), chunk)
        mixed = MID[at_rows, :].astype(jnp.float32) + MR[at_rows, :].astype(jnp.float32)
        middle = (tok[at_rows, :].astype(jnp.float32) + mixed).astype(jnp.bfloat16)
        MID[at_rows, :] = middle
        wide = middle.astype(jnp.float32)
        squares = jnp.sum(wide * wide, axis=1, keepdims=True)
        SQS[0, at_rows, :] = jnp.broadcast_to(squares, (chunk, SQS.shape[2]))

    push(SQS.at[0], SQR.at[0], r_misc.at[2], "c")
    got(SQR.at[0], r_misc.at[2], "sq0")

    @pl.loop(0, rows // chunk)
    def _(i):
        at_rows = pl.ds(pl.multiple_of(i * chunk, chunk), chunk)
        squares = SQS[0, at_rows, 0:1] + SQR[0, at_rows, 0:1]
        scale = lax.rsqrt(squares / width + EPS)
        wide = MID[at_rows, :].astype(jnp.float32)
        normed = (wide * scale * ffn_gain[c]).astype(SN.dtype)
        for l in range(2):
            for v in range(2):
                source = (4 * l + 2 * v) * depth
                target = (4 * v + 2 * l) * depth
                SN[0, 0, at_rows, pl.ds(target, 2 * depth)] = normed[:, source : source + 2 * depth]

    push(SN.at[0, 0], SN.at[2, 0], r_sn.at[2], "zl")
    push(SN.at[0, 0], SN.at[1, 0], r_sn.at[1], "x")
    push(SN.at[0, 0], SN.at[0, 1], r_snc.at[0], "c")

    trade(dn_at, r_dn, dn, trades[0])
    trade(dn_at, r_dn, dn, trades[2])
    for i in (0, 2):
        arrive(gu_at, r_gu, trades[i][0])
        forward(gu_at, r_gu, trades[i][0], ("zh", "y"))
    arrive(gu_at, r_gu, (1, 1, 0, 0))
    forward(gu_at, r_gu, (1, 1, 0, 0), ("y",))
    forward(dn_at, r_dn, mine, ("zh",), dn.at[quarter])
    with jax.named_scope("retire"):
        retire(pool_sent)
    got(SN.at[1, 0], r_sn.at[1], "sn1")
    push(SN.at[1, 0], SN.at[1, 1], r_snc.at[1], "c")
    arrive(dn_at, r_dn, trades[1][0])
    forward(dn_at, r_dn, trades[1][0], ("zh",))
    got(SN.at[2, 0], r_sn.at[2], "sn2")
    push(SN.at[2, 0], SN.at[3, 0], r_sn.at[3], "x")
    push(SN.at[2, 0], SN.at[2, 1], r_snc.at[2], "c")
    locals_[2].wait()
    for which in (trades[0], trades[2]):
        arrive(dn_at, r_dn, which[0])
    for l in range(2):
        forward(dn_at, r_dn, (0, low(l), 0, 1), ("zh",))

    whole_tiles = GU.shape[1] // tile
    half_tile = tile // 2
    lane = lax.broadcasted_iota(jnp.int32, (rows, half_tile), 1)
    near = jnp.where(zh == c, 0, 1)
    near_rows = pl.ds(pl.multiple_of(zh * half, half), half)
    quart = half // 2

    def far_part(v):
        rows_at = pl.multiple_of((1 - zh) * half + v * quart, quart)
        return pl.ds(rows_at, quart), pl.ds(pl.multiple_of(v * quart, quart), quart)

    own_rows_far, own_cols_far = far_part(y)
    end_rows_far, end_cols_far = far_part(1 - y)
    last = pl.ds(whole_tiles * tile, half_tile)

    def tile_at(j, size):
        return pl.ds(pl.multiple_of(j * size, size), size)

    def begin(r):
        got(SN.at[r, 1], r_snc.at[r], f"snc{r}")
        with jax.named_scope(f"begin{r}"):

            @pl.loop(0, whole_tiles)
            def _(j):
                ACC[r, :, tile_at(j, tile)] = dot(SN[r, near], GU[near_rows, tile_at(j, tile)])

            ACC[r, :, last] = dot(SN[r, near], GU[near_rows, last])

    def more(r):
        with jax.named_scope(f"more{r}"):
            left = SN.at[r, 1 - near, :, own_cols_far]

            @pl.loop(0, whole_tiles)
            def _(j):
                here = tile_at(j, tile)
                ACC[r, :, here] = ACC[r, :, here] + dot(left[...], GU[own_rows_far, here])

            ACC[r, :, last] = ACC[r, :, last] + dot(left[...], GU[own_rows_far, last])

    def gated(r):
        left = SN.at[r, 1 - near, :, end_cols_far]
        with jax.named_scope(f"gated{r}"):

            @pl.loop(0, whole_tiles)
            def _(j):
                both = dot(left[...], GU[end_rows_far, tile_at(j, tile)])
                both = both + ACC[r, :, tile_at(j, tile)]
                gate, up = both[:, :half_tile], both[:, half_tile:]
                value = gate / (1.0 + jnp.exp(-gate)) * up
                H[r, :, tile_at(j, half_tile)] = value.astype(H.dtype)

            both = dot(left[...], GU[end_rows_far, last]) + ACC[r, :, last]
            up = pltpu.roll(both, half_tile // 2, 1)
            value = both / (1.0 + jnp.exp(-both)) * up
            H[r, :, pl.ds(whole_tiles * half_tile, half_tile)] = jnp.where(
                lane < half_tile // 2, value, 0.0
            ).astype(H.dtype)

    for b, d in ((0, 0), (0, 1), (1, 0), (1, 1)):
        arrive(gu_at, r_gu, (0, b, 1, d))
    begin(0)
    arrive(gu_at, r_gu, (1, 0, 0, 1))
    forward(gu_at, r_gu, (1, 0, 0, 1), ("y",))
    begin(1)
    begin(2)
    arrive(gu_at, r_gu, (1, 1, 0, 1))
    forward(gu_at, r_gu, (1, 1, 0, 1), ("y",))
    more(0)
    more(1)
    got(SN.at[3, 0], r_sn.at[3], "sn3")
    push(SN.at[3, 0], SN.at[3, 1], r_snc.at[3], "c")
    for l in range(2):
        for u in range(2):
            forward(dn_at, r_dn, (0, low(l), 0, side(u)), ("y",))
    more(2)
    begin(3)
    more(3)
    for b, d in ((0, 0), (0, 1), (1, 0), (1, 1)):
        arrive(gu_at, r_gu, (1, b, 1, d))
    whole_steps = [(a, e, l, None) for a in range(2) for e in range(2) for l in range(2)]
    steps = whole_steps[:-1] + [whole_steps[-1][:3] + (u,) for u in range(2)]
    firsts = ("x", "zl")
    owners = (zh == c, zh != c)
    role_sent = ([], [])

    def role_copy(which, *args):
        src, dst, rsem, *names = args
        copy = remote(src, dst, SENDS + len(role_sent[which]), rsem, *names)
        role_sent[which].append(copy)
        return copy

    def place_of(s):
        a, _, _, u = steps[s]
        slot = min(s - 4 * a, 3)
        start, size = (0, tile) if u is None else (u * half_tile, half_tile)
        return a, slot, s - 4 * a, pl.ds(start, size)

    def step_cols(s, which=0):
        _, e, l, u = steps[s]
        v = y + e * (1 - 2 * y)
        start, size = (0, tile) if u is None else (u * half_tile, half_tile)
        return pl.ds(pl.multiple_of(which * half + (2 * l + v) * tile + start, size), size)

    def produce(s, blocks=(0, 1, 2, 3)):
        a, t, i, part = place_of(s)
        columns = step_cols(s, zh + a * (1 - 2 * zh))
        single = s >= 2
        if single:
            ways = [(TS.at[t, :, :, part], TR.at[t, :, :, part], r_tp.at[tp_index(s)])]
        else:
            ways = [(TS.at[t, r], TR.at[t, r], r_tp.at[tp_index(s) + r]) for r in blocks]
        overs = [role_copy(1 - a, *way, "c") for way in ways]

        @pl.when(owners[1 - a])
        def _():
            for n, r in enumerate(blocks):
                TS[t, r, :, part] = dot(H[r], DN[:, columns]).astype(TS.dtype)
                if not single:
                    overs[n].start()
            if single:
                overs[0].start()

        @pl.when(owners[a])
        def _():
            for r in blocks:
                OWN[t, r, :, part] = dot(H[r], DN[:, columns])

    def tp_index(s):
        a, t, i, part = place_of(s)
        return i if a else (4 * s if s < 2 else 6 + s)

    def crossed(s):
        a, t, i, part = place_of(s)
        got(TR.at[t, :, :, part], r_tp.at[tp_index(s)], f"tp{s}")

    def both_cores(s, r):
        a, t, i, part = place_of(s)
        if s < 2:
            got(TR.at[t, r], r_tp.at[tp_index(s) + r], f"tp{s}r{r}")
        return OWN[t, r, :, part] + TR[t, r, :, part].astype(jnp.float32)

    def halves_of(axis):
        return ((1, 3), (0, 2)) if axis == "x" else ((2, 3), (0, 1))

    def first_stage(s):
        a, t, i, part = place_of(s)
        axis = firsts[s % 2]
        over = role_copy(a, S1.at[t], R1.at[t], r_s1.at[i], axis)

        @pl.when(owners[a])
        def _():
            if s >= 2:
                crossed(s)
            for n, r in enumerate(halves_of(axis)[0]):
                S1[t, n] = both_cores(s, r).astype(S1.dtype)
            over.start()

    def second_stage(s):
        a, t, i, part = place_of(s)
        over = role_copy(a, S2.at[t], R2.at[t], r_s2.at[i], firsts[1 - s % 2])
        keep, give = halves_of(firsts[s % 2])[1]

        @pl.when(owners[a])
        def _():
            given = both_cores(s, give)
            got(R1.at[t], r_s1.at[i], f"first{s}")
            S2[t] = (given + R1[t, 1].astype(jnp.float32)).astype(S2.dtype)
            over.start()
            CL[t] = both_cores(s, keep) + R1[t, 0].astype(jnp.float32)

    def close(s, t, part, columns, summed):
        closing = MID[:, columns].astype(jnp.float32) + summed
        CL[t, :, part] = closing
        squares = jnp.sum(closing * closing, axis=1, keepdims=True)
        squares = jnp.broadcast_to(squares, SQS.shape[1:])
        SQS[1] = squares if t == 0 else SQS[1] + squares

    def finish(s):
        a, t, i, part = place_of(s)
        columns = step_cols(s)

        @pl.when(owners[a])
        def _():
            got(R2.at[t], r_s2.at[i], f"second{s}")
            close(s, t, part, columns, CL[t] + R2[t].astype(jnp.float32))

    def straight(t, part):
        return (
            (3, S2.at[t, :, part], R2.at[t, :, part], r_s2, ("zl", "x")),
            (1, S1.at[t, 0, :, part], R1.at[t, 0, :, part], r_s1, ("x",)),
            (2, S1.at[t, 1, :, part], R1.at[t, 1, :, part], r_s3, ("zl",)),
        )

    def scatter(s):
        a, t, i, part = place_of(s)
        ways = straight(t, part)
        overs = [
            role_copy(a, source, target, sems.at[i], *names)
            for _, source, target, sems, names in ways
        ]

        @pl.when(owners[a])
        def _():
            crossed(s)
            for (r, source, _, _, _), over in zip(ways, overs):
                source[...] = both_cores(s, r).astype(S1.dtype)
                over.start()
            CL[t, :, part] = both_cores(s, 0)

    def gather_sums(s):
        a, t, i, part = place_of(s)
        columns = step_cols(s)

        @pl.when(owners[a])
        def _():
            summed = CL[t, :, part]
            for r, _, target, sems, _ in straight(t, part):
                got(target, sems.at[i], f"sum{s}from{r}")
                summed = summed + target[...].astype(jnp.float32)
            close(s, t, part, columns, summed)

    def relay(l):
        for d in range(2):
            k = (1, low(l, 1), 0, d)
            arrive(dn_at, r_dn, k)
            forward(dn_at, r_dn, k, ("y",))

    def landed(a, l, which=(0, 1)):
        for u in which:
            arrive(dn_at, r_dn, (a, low(l, a), 1, side(u)))

    gated(3)
    gated(1)
    produce(0, (1, 3))
    gated(2)
    produce(1, (2, 3))
    first_stage(0)
    gated(0)
    produce(0, (0, 2))
    produce(1, (0, 1))
    first_stage(1)
    landed(0, 0)
    produce(2)
    relay(0)
    produce(4)
    first_stage(2)
    landed(0, 1)
    produce(3)
    first_stage(4)
    second_stage(0)
    second_stage(1)
    first_stage(3)
    relay(1)
    produce(5)
    first_stage(5)
    landed(1, 0)
    produce(6)
    first_stage(6)
    landed(1, 1, (0,))
    produce(7)
    for s in (2, 3, 4):
        second_stage(s)
    scatter(7)
    second_stage(5)
    landed(1, 1, (1,))
    produce(8)
    scatter(8)
    second_stage(6)
    for s in range(7):
        finish(s)
    for s in (7, 8):
        gather_sums(s)
    push(SQS.at[1], SQR.at[1], r_misc.at[3], "c")
    got(SQR.at[1], r_misc.at[3], "sq1")
    scale = lax.rsqrt((SQS[1, :, 0:1] + SQR[1, :, 0:1]) / width + EPS)
    finals = []
    for t in range(4):
        columns = step_cols(t)
        OUT[:, columns] = (CL[t] * scale * final_gain[:, columns]).astype(out.dtype)
        copy = pltpu.make_async_copy(
            OUT.at[:, columns], out.at[:, columns], local_sems.at[12 + t]
        )
        copy.start()
        finals.append(copy)

    with jax.named_scope("drain"):
        retire(sent)
        for which in range(2):

            @pl.when(owners[which])
            def _():
                for copy in role_sent[which]:
                    copy.wait_send()

        for copy in finals:
            copy.wait()


def fused(
    tokens,
    mixer_gain,
    pool_input,
    group_weight,
    channel_scale,
    pool_output,
    ffn_gain,
    gate_weight,
    up_weight,
    down_weight,
    final_gain,
):
    rows, half = tokens.shape
    depth, hidden_all = gate_weight.shape
    hid = hidden_all // 4
    full = hid // GROUP_DIM
    chans = pool_input.shape[1]
    dn = down_weight.reshape(4, hid, depth)
    pad = (full + 1) * GROUP_DIM
    bf, f32 = jnp.bfloat16, jnp.float32
    hbm = pl.BlockSpec(memory_space=pl.ANY)
    dma = pltpu.SemaphoreType.DMA
    tile = 256
    scratch = [
        pltpu.VMEM((rows, half), bf),
        pltpu.VMEM((1, half), f32),
        pltpu.VMEM((rows, half), bf),
        pltpu.VMEM((2, 1, half), f32),
        pltpu.VMEM(group_weight.shape, bf),
        pltpu.VMEM((1, chans), f32),
        pltpu.VMEM((2, 1, half), f32),
        pltpu.VMEM((2, depth, hidden_all), bf),
        pltpu.VMEM((4, depth, 2 * hid), bf),
        pltpu.VMEM((rows, half), bf),
        pltpu.VMEM((2, rows, half), bf),
        pltpu.VMEM((2 * half, chans), bf),
        pltpu.VMEM((chans, 2 * half), bf),
        pltpu.VMEM((rows, chans), bf),
        pltpu.VMEM((rows, half), bf),
        pltpu.VMEM((rows, half), bf),
        pltpu.VMEM((rows, half), bf),
        pltpu.VMEM((2, rows, GROUP_DIM), f32),
        pltpu.VMEM((2, rows, GROUP_DIM), f32),
        pltpu.VMEM((4, 2, rows, half), bf),
        pltpu.VMEM((2 * half, 2 * hid), bf),
        pltpu.VMEM((pad, 2 * half), bf),
        pltpu.VMEM((4, rows, 2 * hid), f32),
        pltpu.VMEM((4, rows, pad), bf),
        pltpu.VMEM((4, 4, rows, tile), bf),
        pltpu.VMEM((4, 4, rows, tile), bf),
        pltpu.VMEM((4, 4, rows, tile), f32),
        pltpu.VMEM((4, 2, rows, tile), bf),
        pltpu.VMEM((4, 2, rows, tile), bf),
        pltpu.VMEM((4, rows, tile), bf),
        pltpu.VMEM((4, rows, tile), bf),
        pltpu.VMEM((4, rows, tile), f32),
        dma((SENDS + ROLE_SENDS,)),
        dma((16,)),
        dma((PIECES,)),
        dma((PIECES,)),
        dma((PIECES,)),
        dma((PIECES,)),
        dma((4,)),
        dma((4,)),
        dma((4,)),
        dma((10,)),
        dma((5,)),
        dma((5,)),
        dma((5,)),
    ]
    return pl.pallas_call(
        kernel,
        out_shape=jax.ShapeDtypeStruct((rows, half), bf),
        in_specs=[hbm] * 11,
        out_specs=hbm,
        scratch_shapes=scratch,
        compiler_params=pltpu.CompilerParams(
            collective_id=0, has_side_effects=True, vmem_limit_bytes=67043328
        ),
    )(
        tokens,
        mixer_gain.reshape(2, 1, half),
        pool_input,
        group_weight,
        channel_scale.reshape(1, chans),
        pool_output,
        ffn_gain.reshape(2, 1, half),
        gate_weight,
        up_weight,
        dn,
        final_gain.reshape(1, half),
    )


def solution(mesh):
    fs, tp = mesh.shape["fs"], mesh.shape["tp"]
    if fs != PIECES or tp != 2:
        return general(mesh)
    split = Mesh(mesh.devices.reshape(2, 2, 2, 2, 2), AXES)
    rows = AXES[:4]
    placed = (
        P(rows, "c"),
        P(),
        P(rows, "c"),
        P("c", None, None),
        P("c"),
        P("c", rows),
        P(),
        P(rows, "c"),
        P(rows, "c"),
        P("c", rows),
        P("c"),
    )
    return jax.shard_map(
        fused, mesh=split, in_specs=placed, out_specs=P(rows, "c"), check_vma=False
    )
```
